32 devices in a mesh: sp: 8 (over z, y), tp: 4 (over x, core).
Axes of the slice: x: 2, y: 2, z: 4, core: 2. Of those that a mesh axis runs over, the one named last changes fastest.
Arguments:
- resid: bfloat16 [3072, 2048], P('sp', 'tp'), may hold values from -6 to 6
- mixer_in: bfloat16 [3072, 2048], P('sp', 'tp'), may hold values from -6 to 6
- log_step: float32 [3072, 128], P('sp', 'tp'), may hold values from -5.2 to -0.79
- decay_real: float32 [128, 64], P('tp'), may hold values from 0.00016276042 to 0.8
- frequency: float32 [128, 64], P('tp'), may hold values from 0.5 to 6
- input_matrix: float32 [2, 128, 64, 16], P(None, 'tp'), may hold values from -1 to 1
- output_matrix: float32 [2, 128, 16, 64], P(None, 'tp'), may hold values from -0.5 to 0.5
- skip_gain: float32 [2048], P('tp'), may hold values from -4 to 4
- value_weight: bfloat16 [2048, 2048], P(None, 'tp'), may hold values from -0.125 to 0.125
- gate_weight: bfloat16 [2048, 2048], P(None, 'tp'), may hold values from -0.125 to 0.125
- norm_gain: float32 [2048], replicated, may hold values from 0.1 to 1.9
- up_weight: bfloat16 [2048, 8192], P('sp', 'tp'), may hold values from -0.125 to 0.125
- down_weight: bfloat16 [2048, 8192], P('sp', 'tp'), may hold values from -0.0625 to 0.0625
Outputs:
- result: bfloat16 [3072, 2048], P('sp', 'tp')
The draws below stay inside these ranges and needn't reach their ends.
All inputs are finite; a program needn't handle non-finite values.
Results may differ from the reference program's by a relative error of at most 0.014.
Values may be sent and summed in bfloat16 or wider, within the bound.
A program may use at most 128 MiB of HBM per device.

```python
import math
import jax
import jax.numpy as jnp
from jax import lax

D = 2048
FF = 8192
GC = 16
N = 64
TOK_DEV = 384
G = 128
TOKENS = 3072
FF_BLOCK = 2048
N_TP = 4


def draw_log_step(key, part):
    subkeys = jax.random.split(key, 3)
    device_count = TOKENS // TOK_DEV
    device_shift = jax.random.uniform(subkeys[0], (device_count, 1, 1), jnp.float32, -0.7, 0.7)
    group_shift = jax.random.uniform(subkeys[1], (1, 1, G), jnp.float32, -0.5, 0.5)
    jitter = jnp.clip(0.35 * jax.random.normal(subkeys[2], (device_count, TOK_DEV, G), jnp.float32), -1.0, 1.0)
    return (math.log(0.05) + device_shift + group_shift + jitter).reshape(TOKENS, G)


def draw_decay_real(key, part):
    subkeys = jax.random.split(key, 3)
    slow_share = 0.5
    chooser = jax.random.uniform(subkeys[0], (G, N), jnp.float32)
    slow_rate = jnp.exp(jax.random.uniform(subkeys[1], (G, N), jnp.float32, math.log(0.5), math.log(8.0))) / TOKENS
    fast_rate = jnp.exp(jax.random.uniform(subkeys[2], (G, N), jnp.float32, math.log(0.3), math.log(0.8)))
    return jnp.where(chooser < slow_share, slow_rate, fast_rate)


def shard_levels(rng, extent, cuts, smallest, high):
    factor_of = 1.0
    for dim, shards_of in cuts:
        steps = jax.random.uniform(jax.random.fold_in(jax.random.fold_in(rng, 6), dim), (shards_of,), jnp.float32, smallest / len(cuts), high / len(cuts))
        factor_of = factor_of * jnp.repeat(jnp.exp(steps), extent[dim] // shards_of).reshape((-1,) + (1,) * (len(extent) - 1 - dim))
    return factor_of


def normal_values(rng, shape, scale, most, cuts=(), held_as=jnp.bfloat16):
    factor_of = shard_levels(rng, shape, cuts, -0.22, 0.18) if cuts else 1.0
    drawn = jax.random.normal(rng, shape, jnp.float32) * scale * factor_of
    return jnp.minimum(jnp.maximum(drawn, -most), most).astype(held_as)


def setup_inputs(seed: int = 0) -> dict:
    streams_of = jax.random.split(jax.random.key(seed), 14)
    resid = normal_values(streams_of[0], (TOKENS, D), 1.0, 6.0, ((0, 8), (1, 4)))
    mixer_in = normal_values(streams_of[1], (TOKENS, D), 1.0, 6.0, ((0, 8), (1, 4)))
    log_step = draw_log_step(jax.random.fold_in(streams_of[13], 71), 0)
    decay_real = draw_decay_real(jax.random.fold_in(streams_of[13], 71), 0)
    frequency = jnp.clip(0.5 + 5.5 * jax.random.uniform(streams_of[4], (G, N), jnp.float32) ** shard_levels(streams_of[4], (G, N), ((0, 4),), -0.2, 0.2), 0.5, 6.0)
    input_matrix = normal_values(streams_of[5], (2, G, N, GC), (2 * GC) ** -0.5, 1.0, ((1, 4),), jnp.float32)
    output_matrix = normal_values(streams_of[6], (2, G, GC, N), (2 * N) ** -0.5, 0.5, ((1, 4),), jnp.float32)
    skip_gain = normal_values(streams_of[7], (D,), 1.0, 4.0, ((0, 4),), jnp.float32)
    value_weight = normal_values(streams_of[8], (D, D), D ** -0.5, 0.125, ((1, 4),))
    gate_weight = normal_values(streams_of[9], (D, D), D ** -0.5, 0.125, ((1, 4),))
    norm_gain = jnp.clip(1.0 + 0.18 * jax.random.normal(streams_of[10], (D,), jnp.float32), 0.1, 1.9)
    up_weight = normal_values(streams_of[11], (D, FF), D ** -0.5, 0.125, ((0, 8), (1, 4)))
    down_weight = normal_values(streams_of[12], (D, FF), FF ** -0.5, 0.0625, ((0, 8), (1, 4)))
    return dict(resid=resid, mixer_in=mixer_in, log_step=log_step, decay_real=decay_real, frequency=frequency, input_matrix=input_matrix, output_matrix=output_matrix, skip_gain=skip_gain, value_weight=value_weight, gate_weight=gate_weight, norm_gain=norm_gain, up_weight=up_weight, down_weight=down_weight)


rms_eps = 1e-06
highest = lax.Precision.HIGHEST

def chain_link(earlier, later):
    return (earlier[0] * later[0] - earlier[1] * later[1], earlier[0] * later[1] + earlier[1] * later[0], later[0] * earlier[2] - later[1] * earlier[3] + later[2], later[0] * earlier[3] + later[1] * earlier[2] + later[3])

def discretize(log_step, decay_real, frequency):
    states = decay_real.shape[1]
    step_size = jnp.repeat(jnp.exp(log_step), states, axis=1)
    decay_rate = decay_real.reshape(-1)
    angular = frequency.reshape(-1)
    shrink = -decay_rate * step_size
    rotation = angular * step_size
    factor = jnp.exp(shrink)
    decay_re = factor * jnp.cos(rotation)
    decay_im = factor * jnp.sin(rotation)
    half_sine = jnp.sin(0.5 * rotation)
    minus_re = jnp.expm1(shrink) * jnp.cos(rotation) - 2.0 * half_sine * half_sine
    minus_im = decay_im
    modulus = decay_rate * decay_rate + angular * angular
    drive_re = (minus_im * angular - minus_re * decay_rate) / modulus
    drive_im = (-minus_im * decay_rate - minus_re * angular) / modulus
    return (decay_re, decay_im, drive_re, drive_im)

def local_states(mixer_in, log_step, decay_real, frequency, input_matrix):
    tokens = mixer_in.shape[0]
    groups, states = decay_real.shape
    signal = mixer_in.astype(jnp.float32).reshape(tokens, groups, -1)
    proj_re = jnp.einsum('tgk,gnk->tgn', signal, input_matrix[0], precision=highest).reshape(tokens, groups * states)
    proj_im = jnp.einsum('tgk,gnk->tgn', signal, input_matrix[1], precision=highest).reshape(tokens, groups * states)
    decay_re, decay_im, drive_re, drive_im = discretize(log_step, decay_real, frequency)
    feed_re = drive_re * proj_re - drive_im * proj_im
    feed_im = drive_re * proj_im + drive_im * proj_re
    return lax.associative_scan(chain_link, (decay_re, decay_im, feed_re, feed_im), axis=0)

def read_out(state_re, state_im, output_matrix):
    tokens = state_re.shape[0]
    groups = output_matrix.shape[1]
    grid_re = state_re.reshape(tokens, groups, -1)
    grid_im = state_im.reshape(tokens, groups, -1)
    output = jnp.einsum('tgn,gkn->tgk', grid_re, output_matrix[0], precision=highest)
    output = output - jnp.einsum('tgn,gkn->tgk', grid_im, output_matrix[1], precision=highest)
    return output.reshape(tokens, -1)

def reference(resid, mixer_in, log_step, decay_real, frequency, input_matrix, output_matrix, skip_gain, value_weight, gate_weight, norm_gain, up_weight, down_weight):
    group_span = G // N_TP

    def one_block(block_index):
        first_group = block_index * group_span
        columns = lax.dynamic_slice_in_dim(mixer_in, first_group * GC, group_span * GC, 1)
        steps_part = lax.dynamic_slice_in_dim(log_step, first_group, group_span, 1)
        decay_part = lax.dynamic_slice_in_dim(decay_real, first_group, group_span, 0)
        angular = lax.dynamic_slice_in_dim(frequency, first_group, group_span, 0)
        matrix_in = lax.dynamic_slice_in_dim(input_matrix, first_group, group_span, 1)
        matrix_out = lax.dynamic_slice_in_dim(output_matrix, first_group, group_span, 1)
        _, _, state_re, state_im = local_states(columns, steps_part, decay_part, angular, matrix_in)
        return read_out(state_re, state_im, matrix_out)
    outputs = lax.map(one_block, jnp.arange(N_TP, dtype=jnp.int32))
    mechanism = jnp.transpose(outputs, (1, 0, 2)).reshape(TOKENS, D) + skip_gain * mixer_in.astype(jnp.float32)
    mixed_out = jax.nn.gelu(mechanism).astype(jnp.bfloat16)
    value_pre = jnp.dot(mixed_out, value_weight, preferred_element_type=jnp.float32)
    gate_pre = jnp.dot(mixed_out, gate_weight, preferred_element_type=jnp.float32)
    updated = (resid.astype(jnp.float32) + value_pre * jax.nn.sigmoid(gate_pre)).astype(jnp.bfloat16)
    updated_wide = lax.optimization_barrier(updated).astype(jnp.float32)
    inv_rms = lax.rsqrt(lax.optimization_barrier(jnp.mean(updated_wide * updated_wide, axis=1, keepdims=True)) + rms_eps)
    normed = (updated_wide * inv_rms * norm_gain).astype(jnp.bfloat16)
    raised = jnp.dot(normed, up_weight, preferred_element_type=jnp.float32)
    active = jax.nn.relu(raised)
    hidden = (active * active).astype(jnp.bfloat16)

    def add_block(running, block_index):
        start_unit = block_index * FF_BLOCK
        hidden_part = lax.dynamic_slice_in_dim(hidden, start_unit, FF_BLOCK, 1)
        weight_part = lax.dynamic_slice_in_dim(down_weight, start_unit, FF_BLOCK, 1)
        product = lax.dot_general(hidden_part, weight_part, (((1,), (1,)), ((), ())), preferred_element_type=jnp.float32).astype(jnp.bfloat16)
        product = lax.optimization_barrier(product)
        return (running + product.astype(jnp.float32), None)
    down_sum, _ = lax.scan(add_block, jnp.zeros((TOKENS, D), jnp.float32), jnp.arange(N_TP, dtype=jnp.int32))
    return (updated_wide + down_sum).astype(jnp.bfloat16)
```

```python
import functools

import jax
import jax.numpy as jnp
import numpy as np
from jax import lax
from jax.experimental import pallas as pl
from jax.experimental.pallas import tpu as pltpu
from jax.sharding import PartitionSpec as P

rms_eps = 1e-06
segments = 8
MESH = pl.DeviceIdType.MESH
f32, bf16 = jnp.float32, jnp.bfloat16


def sine_cosine(x):
    y = x * x
    s = 1.0 + y * (-1 / 6 + y * (1 / 120 + y * (-1 / 5040 + y * (1 / 362880 + y * (-1 / 39916800)))))
    c = 1.0 + y * (
        -0.5
        + y * (1 / 24 + y * (-1 / 720 + y * (1 / 40320 + y * (-1 / 3628800 + y * (1 / 479001600)))))
    )
    return x * s, c


def expm1_small(y):
    return y * (
        1.0
        + y * (1 / 2 + y * (1 / 6 + y * (1 / 24 + y * (1 / 120 + y * (1 / 720 + y * (1 / 5040))))))
    )


def kernel(
    n,
    ntp,
    resid_ref,
    mixer_ref,
    step_ref,
    decay_ref,
    angle_ref,
    w_in_ref,
    w_out_ref,
    skip_ref,
    value_hbm,
    gate_hbm,
    gain_ref,
    up_hbm,
    down_hbm,
    perm_ref,
    unperm_ref,
    out_ref,
    up_whole,
    down_whole,
    value_ref,
    gate_ref,
    dre,
    dim,
    fre,
    fim,
    step_wide,
    proj,
    ends,
    carries,
    entry,
    mixer_perm,
    chan,
    upd,
    normed,
    hidden,
    keep,
    out1,
    in1,
    out2,
    in2,
    out3,
    in3,
    own_sem,
    z_send,
    z_recv,
    y_send,
    y_recv,
    carry_send,
    carry_recv,
    chan_core_send,
    chan_core_recv,
    chan_x_send,
    chan_x_recv,
    upd_z_send,
    upd_z_recv,
    upd_core_send,
    upd_core_recv,
    upd_x_send,
    upd_x_recv,
    sum1_send,
    sum1_recv,
    sum2_send,
    sum2_recv,
    sum3_send,
    sum3_recv,
):
    sp = lax.axis_index("sp")
    tp = lax.axis_index("tp")
    tokens, width = mixer_ref.shape
    block = up_hbm.shape[0]
    units = up_whole.shape[1]
    groups, states = decay_ref.shape
    each = width // groups
    bunch = min(128 // each, groups)
    chunks = groups // bunch
    lanes, kin = bunch * states, bunch * each
    length = tokens // segments
    pieces = z_send.shape[2]
    piece = block // pieces
    nz, nx, per = n // 2, ntp // 2, n // ntp
    z, y = sp // 2, sp % 2
    x, core = tp // 2, tp % 2
    partner = tp + 1 - 2 * core

    def xor(a, k):
        total = 0
        bit = 1
        while bit < nz:
            digit = (a // bit) % 2
            total = total + bit * (1 - digit if k & bit else digit)
            bit *= 2
        return total

    def flip(a):
        return a + 1 - 2 * (a % 2)

    pair_z = flip(z)
    pair = 2 * pair_z + y
    inner = ((z + 1) // 2) % 2

    barrier = pltpu.get_barrier_semaphore()
    for i in range(1, n):
        pl.semaphore_signal(barrier, inc=1, device_id=((sp + i) % n, tp), device_id_type=MESH)
    for i in range(1, ntp):
        pl.semaphore_signal(barrier, inc=1, device_id=(sp, (tp + i) % ntp), device_id_type=MESH)
    pl.semaphore_wait(barrier, n - 1 + ntp - 1)

    sources, wholes = (up_hbm, down_hbm), (up_whole, down_whole)

    def rows_of(owner, part=None):
        if part is None:
            return pl.ds(pl.multiple_of(owner * block, block), block)
        return pl.ds(pl.multiple_of(owner * block + part * piece, piece), piece)

    def columns_for(a):
        return pl.ds(pl.multiple_of((a % 2) * units, units), units)

    def z_copy(which, k, zk, part, sending):
        owner = sp if sending else 2 * zk + y
        return pltpu.make_async_remote_copy(
            src_ref=sources[which].at[pl.ds(part * piece, piece), columns_for(zk)],
            dst_ref=wholes[which].at[rows_of(owner, part)],
            send_sem=z_send.at[which, k, part],
            recv_sem=z_recv.at[which, k, part],
            device_id=(2 * zk + y, tp),
            device_id_type=MESH,
        )

    def y_copy(which, k, zk, part, sending):
        owner = 2 * zk + (y if sending else 1 - y)
        slot = wholes[which].at[rows_of(owner, part)]
        src = slot
        if isinstance(k, int) and k == 0:
            src = sources[which].at[pl.ds(part * piece, piece), columns_for(z)]
        return pltpu.make_async_remote_copy(
            src_ref=src,
            dst_ref=slot,
            send_sem=y_send.at[which, k, part],
            recv_sem=y_recv.at[which, k, part],
            device_id=(2 * z + 1 - y, tp),
            device_id_type=MESH,
        )

    def z_start(which, k):
        for part in range(pieces):
            z_copy(which, k, xor(z, k), part, True).start()

    def forward(which, k, zk):
        for part in range(pieces):
            z_copy(which, k, zk, part, False).wait_recv()
            y_copy(which, k, zk, part, True).start()

    def y_arrived(which, k, zk):
        for part in range(pieces):
            y_copy(which, k, zk, part, False).wait_recv()

    far = []
    for base in range(2, nz, 2):
        zb = xor(z, base)
        zf = flip(zb)
        far.append((base + inner, zb + inner * (zf - zb)))
        far.append((base + 1 - inner, zf + inner * (zb - zf)))
    near, distant = far[0::2], far[1::2]

    own = []
    for which in range(2):
        c = pltpu.make_async_copy(
            sources[which].at[:, columns_for(z)], wholes[which].at[rows_of(sp)], own_sem.at[which]
        )
        c.start()
        own.append(c)
    for which in range(2):
        for part in range(pieces):
            y_copy(which, 0, z, part, True).start()
        z_start(which, 1)
    for k in range(2, nz):
        z_start(0, k)
    gates = []
    for which, (source, target) in enumerate(((value_hbm, value_ref), (gate_hbm, gate_ref))):
        c = pltpu.make_async_copy(source, target, own_sem.at[2 + which])
        c.start()
        gates.append(c)

    def far_down():
        for k in range(2, nz):
            z_start(1, k)

    def tp_at(a, b):
        return 2 * a + b

    def chan_core(i, c, sending):
        cols = pl.ds(c * kin, kin)
        slot = tp_at((x + nx - i) % nx, core if sending else 1 - core)
        return pltpu.make_async_remote_copy(
            src_ref=chan.at[slot, :, cols],
            dst_ref=chan.at[slot, :, cols],
            send_sem=chan_core_send.at[i, c],
            recv_sem=chan_core_recv.at[i, c],
            device_id=(sp, partner),
            device_id_type=MESH,
        )

    def chan_x(i, c, sending):
        cols = pl.ds(c * kin, kin)
        slot = tp if sending else tp_at((x + nx - i) % nx, core)
        return pltpu.make_async_remote_copy(
            src_ref=chan.at[slot, :, cols],
            dst_ref=chan.at[slot, :, cols],
            send_sem=chan_x_send.at[i - 1, c],
            recv_sem=chan_x_recv.at[i - 1, c],
            device_id=(sp, tp_at((x + i) % nx, core)),
            device_id_type=MESH,
        )

    def chan_forward(c):
        for i in range(1, nx):
            chan_x(i, c, False).wait_recv()
            chan_core(i, c, True).start()

    mixer_perm[...] = jnp.dot(
        perm_ref[...], mixer_ref[...], preferred_element_type=f32
    ).astype(bf16)
    highest = lax.Precision.HIGHEST
    step_size = lax.dot_general(
        perm_ref[...].astype(f32),
        jnp.exp(step_ref[...]),
        (((1,), (1,)), ((), ())),
        precision=highest,
        preferred_element_type=f32,
    )

    def iota(shape, axis):
        return lax.broadcasted_iota(jnp.int32, shape, axis)

    def ones_where(mask, dtype=f32):
        return jnp.where(mask, 1.0, 0.0).astype(dtype)

    def belongs(rows, columns, span, first):
        gap = iota((rows, columns), 1) + first - iota((rows, columns), 0) * span
        return ones_where((gap >= 0) & (gap < span))

    def tiled(size, copies):
        shape = (size, size * copies)
        hits = jnp.zeros(shape, f32)
        for i in range(copies):
            hits += ones_where(iota(shape, 1) - iota(shape, 0) == i * size)
        return hits

    over_states = tiled(states, bunch)
    agree = jnp.zeros((kin, lanes), f32)
    for i in range(bunch):
        r, l = iota((kin, lanes), 0) - i * each, iota((kin, lanes), 1) - i * states
        agree += ones_where((r >= 0) & (r < each) & (l >= 0) & (l < states))

    def wide_rate(table, c):
        spread = jnp.dot(table, over_states, precision=highest, preferred_element_type=f32)
        return jnp.sum(
            spread * belongs(groups, lanes, states, c * lanes), axis=0, keepdims=True
        )

    for c in range(chunks):
        cols = pl.ds(c * lanes, lanes)
        step_wide[...] = jnp.dot(
            step_size,
            belongs(groups, lanes, states, c * lanes),
            precision=highest,
            preferred_element_type=f32,
        )
        for i in range(2):
            matrix = jnp.dot(
                w_in_ref[i, c * kin : (c + 1) * kin, :].astype(bf16),
                over_states.astype(bf16),
                preferred_element_type=f32,
            )
            proj[:, i * lanes : (i + 1) * lanes] = jnp.dot(
                mixer_perm[:, c * kin : (c + 1) * kin],
                (matrix * agree).astype(bf16),
                preferred_element_type=f32,
            )
        rate_row = wide_rate(decay_ref[...], c)
        angle_row = wide_rate(angle_ref[...], c)
        modulus = rate_row * rate_row + angle_row * angle_row
        shape = (segments, lanes)
        rate = jnp.broadcast_to(rate_row, shape)
        half_angle = jnp.broadcast_to(angle_row * 0.5, shape)
        rate_n = jnp.broadcast_to(rate_row / modulus, shape)
        angle_n = jnp.broadcast_to(angle_row / modulus, shape)

        def one(j, state):
            pr, pi, sr, si = state
            rows = pl.ds(pl.multiple_of(j * segments, segments), segments)
            step = step_wide[rows, :]
            s, co = sine_cosine(half_angle * step)
            em = expm1_small(-rate * step)
            factor = 1.0 + em
            twice = 2.0 * s * s
            cos_r = 1.0 - twice
            dr = factor * cos_r
            di = factor * (2.0 * s * co)
            mr = em * cos_r - twice
            vr = di * angle_n - mr * rate_n
            vi = -di * rate_n - mr * angle_n
            a = proj[rows, 0:lanes]
            b = proj[rows, lanes : 2 * lanes]
            fr = vr * a - vi * b
            fi = vr * b + vi * a
            dre[rows, cols] = dr
            dim[rows, cols] = di
            fre[rows, cols] = fr
            fim[rows, cols] = fi
            return (
                dr * pr - di * pi,
                dr * pi + di * pr,
                dr * sr - di * si + fr,
                dr * si + di * sr + fi,
            )

        zero = jnp.zeros(shape, f32)
        last = lax.fori_loop(0, length, one, (zero + 1.0, zero, zero, zero), unroll=2)
        for i in range(4):
            ends[i, :, cols] = last[i]
        if c >= chunks - 2:
            forward(c - chunks + 2, 1, pair_z)

    def link(earlier, later):
        return (
            later[0] * earlier[0] - later[1] * earlier[1] + later[2],
            later[0] * earlier[1] + later[1] * earlier[0] + later[3],
        )

    pr, pi, sr, si = (ends[i, 0:1, :] for i in range(4))
    for s in range(1, segments):
        qr, qi, tr, ti = (ends[i, s : s + 1, :] for i in range(4))
        pr, pi = qr * pr - qi * pi, qr * pi + qi * pr
        sr, si = link((sr, si), (qr, qi, tr, ti))
    for i, v in enumerate((pr, pi, sr, si)):
        carries[sp, i : i + 1, :] = v

    def carry_copy(i, sending):
        there = (sp + i) % n
        slot = sp if sending else (sp + n - i) % n
        return pltpu.make_async_remote_copy(
            src_ref=carries.at[slot],
            dst_ref=carries.at[slot],
            send_sem=carry_send.at[i - 1],
            recv_sem=carry_recv.at[i - 1],
            device_id=(there, tp),
            device_id_type=MESH,
        )

    for i in range(1, n):
        carry_copy(i, True).start()
    for i in range(1, n):
        carry_copy(i, False).wait_recv()
    cr = jnp.zeros_like(pr)
    ci = jnp.zeros_like(pr)
    for d in range(n - 1):
        nr, ni = link((cr, ci), tuple(carries[d, i : i + 1, :] for i in range(4)))
        cr = jnp.where(d < sp, nr, cr)
        ci = jnp.where(d < sp, ni, ci)
    for s in range(segments):
        entry[0, s : s + 1, :] = cr
        entry[1, s : s + 1, :] = ci
        cr, ci = link((cr, ci), tuple(ends[i, s : s + 1, :] for i in range(4)))

    for c in range(chunks):
        cols = pl.ds(c * lanes, lanes)

        def again(j, state):
            rows = pl.ds(pl.multiple_of(j * segments, segments), segments)
            dr, di = dre[rows, cols], dim[rows, cols]
            xr, xi = link(state, (dr, di, fre[rows, cols], fim[rows, cols]))
            proj[rows, 0:lanes] = xr
            proj[rows, lanes : 2 * lanes] = xi
            return xr, xi

        lax.fori_loop(0, length, again, (entry[0, :, cols], entry[1, :, cols]), unroll=4)
        ins = slice(c * kin, (c + 1) * kin)
        mech = jnp.zeros((tokens, kin), f32)
        for i in range(2):
            matrix = jnp.dot(
                w_out_ref[i, c * kin : (c + 1) * kin, :].astype(bf16),
                over_states.astype(bf16),
                preferred_element_type=f32,
            )
            mech += (1 - 2 * i) * lax.dot_general(
                proj[:, i * lanes : (i + 1) * lanes].astype(bf16),
                (matrix * agree).astype(bf16),
                (((1,), (1,)), ((), ())),
                preferred_element_type=f32,
            )
        mech = mech + skip_ref[0:1, ins] * mixer_perm[:, ins].astype(f32)
        mixed = jax.nn.gelu(mech).astype(bf16)
        chan[tp, :, ins] = jnp.dot(
            unperm_ref[...], mixed, preferred_element_type=f32
        ).astype(bf16)
        chan_core(0, c, True).start()
        for i in range(1, nx):
            chan_x(i, c, True).start()
        if c >= 2:
            chan_forward(c - 2)

    @pl.when(inner == 1)
    def _():
        far_down()

    for k, zk in near + distant:
        forward(0, k, zk)
    for c in range(max(chunks - 2, 0), chunks):
        chan_forward(c)
    for c in gates:
        c.wait()
    for c in range(chunks):
        for i in range(nx):
            chan_core(i, c, False).wait_recv()

    tile = 256

    @pl.loop(0, width // tile)
    def _(t):
        cols = pl.ds(pl.multiple_of(t * tile, tile), tile)
        v = jnp.zeros((tokens, tile), f32)
        g = jnp.zeros((tokens, tile), f32)
        for q in range(ntp):
            rows = slice(q * width, (q + 1) * width)
            v += jnp.dot(chan[q], value_ref[rows, cols], preferred_element_type=f32)
            g += jnp.dot(chan[q], gate_ref[rows, cols], preferred_element_type=f32)
        upd[0, tp, :, cols] = (resid_ref[:, cols].astype(f32) + v * jax.nn.sigmoid(g)).astype(bf16)

    def upd_z():
        return pltpu.make_async_remote_copy(
            src_ref=upd.at[0, tp],
            dst_ref=upd.at[1, tp],
            send_sem=upd_z_send.at[0],
            recv_sem=upd_z_recv.at[0],
            device_id=(pair, tp),
            device_id_type=MESH,
        )

    def upd_x(i, h, sending):
        slot = tp if sending else tp_at((x + nx - i) % nx, core)
        return pltpu.make_async_remote_copy(
            src_ref=upd.at[h, slot],
            dst_ref=upd.at[h, slot],
            send_sem=upd_x_send.at[i - 1, h],
            recv_sem=upd_x_recv.at[i - 1, h],
            device_id=(sp, tp_at((x + i) % nx, core)),
            device_id_type=MESH,
        )

    def upd_core(i, h, sending):
        slot = tp_at((x + nx - i) % nx, core if sending else 1 - core)
        return pltpu.make_async_remote_copy(
            src_ref=upd.at[h, slot],
            dst_ref=upd.at[h, slot],
            send_sem=upd_core_send.at[i, h],
            recv_sem=upd_core_recv.at[i, h],
            device_id=(sp, partner),
            device_id_type=MESH,
        )

    upd_z().start()
    for i in range(1, nx):
        upd_x(i, 0, True).start()
    upd_core(0, 0, True).start()

    @pl.when(inner == 0)
    def _():
        far_down()

    for i in range(1, nx):
        upd_x(i, 0, False).wait_recv()
        upd_core(i, 0, True).start()
    upd_z().wait_recv()
    for i in range(1, nx):
        upd_x(i, 1, True).start()
    upd_core(0, 1, True).start()

    def normalize(h):
        for i in range(nx):
            upd_core(i, h, False).wait_recv()
        total = jnp.zeros((tokens, 1), f32)
        for q in range(ntp):
            u = upd[h, q].astype(f32)
            total += jnp.sum(u * u, axis=1, keepdims=True)
        inv = lax.rsqrt(total * (1.0 / (width * ntp)) + rms_eps)
        for q in range(ntp):
            cols = slice(q * width, (q + 1) * width)
            normed[:, cols] = (upd[h, q].astype(f32) * inv * gain_ref[0:1, cols]).astype(bf16)

    def raise_up(h):
        @pl.loop(0, units // tile)
        def _(t):
            cols = pl.ds(pl.multiple_of(t * tile, tile), tile)
            r = jnp.dot(normed[...], up_whole[:, cols], preferred_element_type=f32)
            r = jnp.maximum(r, 0.0)
            hidden[h * tokens : (h + 1) * tokens, cols] = (r * r).astype(bf16)

    normalize(0)
    for c in own:
        c.wait()
    y_arrived(0, 0, z)
    y_arrived(0, 1, pair_z)
    for k, zk in far:
        y_arrived(0, k, zk)
    raise_up(0)
    for i in range(1, nx):
        upd_x(i, 1, False).wait_recv()
        upd_core(i, 1, True).start()
    normalize(1)
    raise_up(1)

    def sum1(s):
        return pltpu.make_async_remote_copy(
            src_ref=out1.at[s],
            dst_ref=in1.at[s],
            send_sem=sum1_send.at[s],
            recv_sem=sum1_recv.at[s],
            device_id=(sp, partner),
            device_id_type=MESH,
        )

    def sum2(s):
        return pltpu.make_async_remote_copy(
            src_ref=out2.at[s],
            dst_ref=in2.at[s % per, x],
            send_sem=sum2_send.at[s],
            recv_sem=sum2_recv.at[s % per, x],
            device_id=(sp, s // per),
            device_id_type=MESH,
        )

    def sum3(j):
        return pltpu.make_async_remote_copy(
            src_ref=out3.at[j],
            dst_ref=in3.at[j],
            send_sem=sum3_send.at[j],
            recv_sem=sum3_recv.at[j],
            device_id=(pair, tp),
            device_id_type=MESH,
        )

    def core_of(s):
        return (s // per) % 2

    def x_of(s):
        return s // per // 2

    def stage1(s):
        rows = rows_of(s)

        @pl.loop(0, 2)
        def _(h):
            some = pl.ds(pl.multiple_of(h * tokens, tokens), tokens)
            keep[s, some, :] = lax.dot_general(
                hidden[some, :],
                down_whole[rows, :],
                (((1,), (1,)), ((), ())),
                preferred_element_type=f32,
            )

        @pl.when(core_of(s) != core)
        def _():
            out1[s] = keep[s].astype(bf16)
            sum1(s).start()

    def stage2(s):
        @pl.when(core_of(s) == core)
        def _():
            sum1(s).wait_recv()
            total = keep[s] + in1[s].astype(f32)

            @pl.when(x_of(s) == x)
            def _():
                keep[s] = total

            @pl.when(x_of(s) != x)
            def _():
                out2[s] = total.astype(bf16)
                sum2(s).start()

    def stage3(s):
        j = s % per

        @pl.when(s // per == tp)
        def _():
            total = keep[s]
            for i in range(1, nx):
                there = (x + i) % nx
                pltpu.make_async_remote_copy(
                    src_ref=out2.at[s],
                    dst_ref=in2.at[j, there],
                    send_sem=sum2_send.at[s],
                    recv_sem=sum2_recv.at[j, there],
                    device_id=(sp, tp_at(there, core)),
                    device_id_type=MESH,
                ).wait_recv()
                total += in2[j, there].astype(f32)
            keep[s] = total
            out3[j] = total[tokens:].astype(bf16)
            sum3(j).start()

    order = []

    def step(k, zk, side):
        if side == 1:
            y_arrived(1, k, zk)
        s = 2 * zk + (y if side == 0 else 1 - y)
        stage1(s)
        order.append(s)
        if len(order) > 1:
            stage2(order[-2])
        if len(order) > 3:
            stage3(order[-4])

    for k, zk in near:
        forward(1, k, zk)
    for side in range(2):
        step(0, z, side)
    for side in range(2):
        step(1, pair_z, side)
    for k, zk in near:
        for side in range(2):
            step(k, zk, side)
    for k, zk in distant:
        forward(1, k, zk)
    for k, zk in distant:
        for side in range(2):
            step(k, zk, side)
    stage2(order[-1])
    for s in order[-3:]:
        stage3(s)
    for j in range(per):
        s = tp * per + j
        sum3(j).wait_recv()
        cols = slice(j * block, (j + 1) * block)
        total = keep[s, :tokens] + in3[j].astype(f32)
        out_ref[:, cols] = (upd[0, tp, :, cols].astype(f32) + total).astype(bf16)

    for which in range(2):
        for k in range(nz):
            for part in range(pieces):
                y_copy(which, k, xor(z, k), part, True).wait_send()
                if k > 0:
                    z_copy(which, k, xor(z, k), part, True).wait_send()
    for i in range(1, n):
        carry_copy(i, True).wait_send()
    for i in range(nx):
        for c in range(chunks):
            chan_core(i, c, True).wait_send()
            if i > 0:
                chan_x(i, c, True).wait_send()
        for h in range(2):
            upd_core(i, h, True).wait_send()
            if i > 0:
                upd_x(i, h, True).wait_send()
    upd_z().wait_send()
    for s in range(n):

        @pl.when(core_of(s) != core)
        def _():
            sum1(s).wait_send()

        @pl.when((core_of(s) == core) & (x_of(s) != x))
        def _():
            sum2(s).wait_send()

    for j in range(per):
        sum3(j).wait_send()


def per_device(
    n,
    ntp,
    resid,
    mixer_in,
    log_step,
    decay_real,
    frequency,
    input_matrix,
    output_matrix,
    skip_gain,
    value_weight,
    gate_weight,
    norm_gain,
    up_weight,
    down_weight,
):
    tokens, width = mixer_in.shape
    groups, states = decay_real.shape
    each = width // groups
    bunch = min(128 // each, groups)
    chunks = groups // bunch
    lanes = bunch * states
    features, units = value_weight.shape[0], up_weight.shape[1] // 2
    block = up_weight.shape[0]
    length = tokens // segments
    row = np.arange(tokens)
    perm = (row[None, :] == ((row % segments) * length + row // segments)[:, None]).astype(np.float32)
    nz, nx, per, pieces = n // 2, ntp // 2, n // ntp, 2
    total = groups * states
    dma = pltpu.SemaphoreType.DMA
    vmem = pl.BlockSpec(memory_space=pltpu.VMEM)
    hbm = pl.BlockSpec(memory_space=pl.ANY)
    return pl.pallas_call(
        functools.partial(kernel, n, ntp),
        out_shape=jax.ShapeDtypeStruct((tokens, width), bf16),
        in_specs=[vmem] * 8 + [hbm] * 2 + [vmem] + [hbm] * 2 + [vmem] * 2,
        out_specs=vmem,
        scratch_shapes=[
            pltpu.VMEM((features, units), bf16),
            pltpu.VMEM((features, units), bf16),
            pltpu.VMEM((features, width), bf16),
            pltpu.VMEM((features, width), bf16),
            pltpu.VMEM((tokens, total), f32),
            pltpu.VMEM((tokens, total), f32),
            pltpu.VMEM((tokens, total), f32),
            pltpu.VMEM((tokens, total), f32),
            pltpu.VMEM((tokens, lanes), f32),
            pltpu.VMEM((tokens, 2 * lanes), f32),
            pltpu.VMEM((4, segments, total), f32),
            pltpu.VMEM((n, 4, total), f32),
            pltpu.VMEM((2, segments, total), f32),
            pltpu.VMEM((tokens, width), bf16),
            pltpu.VMEM((ntp, tokens, width), bf16),
            pltpu.VMEM((2, ntp, tokens, width), bf16),
            pltpu.VMEM((tokens, features), bf16),
            pltpu.VMEM((2 * tokens, units), bf16),
            pltpu.VMEM((n, 2 * tokens, block), f32),
            pltpu.VMEM((n, 2 * tokens, block), bf16),
            pltpu.VMEM((n, 2 * tokens, block), bf16),
            pltpu.VMEM((n, 2 * tokens, block), bf16),
            pltpu.VMEM((per, nx, 2 * tokens, block), bf16),
            pltpu.VMEM((per, tokens, block), bf16),
            pltpu.VMEM((per, tokens, block), bf16),
            dma((4,)),
            dma((2, nz, pieces)),
            dma((2, nz, pieces)),
            dma((2, nz, pieces)),
            dma((2, nz, pieces)),
            dma((n - 1,)),
            dma((n - 1,)),
            dma((nx, chunks)),
            dma((nx, chunks)),
            dma((max(nx - 1, 1), chunks)),
            dma((max(nx - 1, 1), chunks)),
            dma((1,)),
            dma((1,)),
            dma((nx, 2)),
            dma((nx, 2)),
            dma((max(nx - 1, 1), 2)),
            dma((max(nx - 1, 1), 2)),
            dma((n,)),
            dma((n,)),
            dma((n,)),
            dma((per, nx)),
            dma((per,)),
            dma((per,)),
        ],
        compiler_params=pltpu.CompilerParams(
            collective_id=0, has_side_effects=True, vmem_limit_bytes=64 * 1024 * 1024 - 65536
        ),
    )(
        resid,
        mixer_in,
        log_step.T,
        decay_real,
        frequency,
        jnp.transpose(input_matrix, (0, 1, 3, 2)).reshape(2, width, states),
        output_matrix.reshape(2, width, states),
        skip_gain.reshape(1, width),
        value_weight,
        gate_weight,
        norm_gain.reshape(1, features),
        up_weight,
        down_weight,
        jnp.asarray(perm, bf16),
        jnp.asarray(perm.T, bf16),
    )


def solution(mesh):
    in_specs = (
        P("sp", "tp"),
        P("sp", "tp"),
        P("sp", "tp"),
        P("tp", None),
        P("tp", None),
        P(None, "tp", None, None),
        P(None, "tp", None, None),
        P("tp"),
        P(None, "tp"),
        P(None, "tp"),
        P(),
        P("sp", "tp"),
        P("sp", "tp"),
    )
    body = functools.partial(per_device, mesh.shape["sp"], mesh.shape["tp"])
    return jax.shard_map(
        body, mesh=mesh, in_specs=in_specs, out_specs=P("sp", "tp"), check_vma=False
    )
```

```python
import functools

import jax
import jax.numpy as jnp
import numpy as np
from jax import lax
from jax.experimental import pallas as pl
from jax.experimental.pallas import tpu as pltpu
from jax.sharding import PartitionSpec as P

rms_eps = 1e-06
segments = 8
MESH = pl.DeviceIdType.MESH
f32, bf16 = jnp.float32, jnp.bfloat16


def sine_cosine(x):
    y = x * x
    s = 1.0 + y * (-1 / 6 + y * (1 / 120 + y * (-1 / 5040 + y * (1 / 362880 + y * (-1 / 39916800)))))
    c = 1.0 + y * (
        -0.5
        + y * (1 / 24 + y * (-1 / 720 + y * (1 / 40320 + y * (-1 / 3628800 + y * (1 / 479001600)))))
    )
    return x * s, c


def expm1_small(y):
    return y * (
        1.0
        + y * (1 / 2 + y * (1 / 6 + y * (1 / 24 + y * (1 / 120 + y * (1 / 720 + y * (1 / 5040))))))
    )


def kernel(
    n,
    ntp,
    resid_ref,
    mixer_ref,
    step_ref,
    decay_ref,
    angle_ref,
    w_in_ref,
    w_out_ref,
    skip_ref,
    value_hbm,
    gate_hbm,
    gain_ref,
    up_hbm,
    down_hbm,
    perm_ref,
    unperm_ref,
    out_ref,
    up_whole,
    down_whole,
    value_ref,
    gate_ref,
    dre,
    dim,
    fre,
    fim,
    step_wide,
    proj,
    ends,
    carries,
    entry,
    mixer_perm,
    chan,
    upd,
    normed,
    hidden,
    keep,
    out1,
    in1,
    out2,
    in2,
    out3,
    in3,
    own_sem,
    z_send,
    z_recv,
    y_send,
    y_recv,
    carry_send,
    carry_recv,
    chan_core_send,
    chan_core_recv,
    chan_x_send,
    chan_x_recv,
    upd_z_send,
    upd_z_recv,
    upd_core_send,
    upd_core_recv,
    upd_x_send,
    upd_x_recv,
    sum1_send,
    sum1_recv,
    sum2_send,
    sum2_recv,
    sum3_send,
    sum3_recv,
):
    sp = lax.axis_index("sp")
    tp = lax.axis_index("tp")
    tokens, width = mixer_ref.shape
    block = up_hbm.shape[0]
    units = up_whole.shape[1]
    groups, states = decay_ref.shape
    each = width // groups
    bunch = min(128 // each, groups)
    chunks = groups // bunch
    lanes, kin = bunch * states, bunch * each
    length = tokens // segments
    pieces = z_send.shape[2]
    piece = block // pieces
    nz, nx, per = n // 2, ntp // 2, n // ntp
    z, y = sp // 2, sp % 2
    x, core = tp // 2, tp % 2
    partner = tp + 1 - 2 * core

    def xor(a, k):
        total = 0
        bit = 1
        while bit < nz:
            digit = (a // bit) % 2
            total = total + bit * (1 - digit if k & bit else digit)
            bit *= 2
        return total

    def flip(a):
        return a + 1 - 2 * (a % 2)

    pair_z = flip(z)
    pair = 2 * pair_z + y
    inner = ((z + 1) // 2) % 2

    barrier = pltpu.get_barrier_semaphore()
    for i in range(1, n):
        pl.semaphore_signal(barrier, inc=1, device_id=((sp + i) % n, tp), device_id_type=MESH)
    for i in range(1, ntp):
        pl.semaphore_signal(barrier, inc=1, device_id=(sp, (tp + i) % ntp), device_id_type=MESH)
    pl.semaphore_wait(barrier, n - 1 + ntp - 1)

    sources, wholes = (up_hbm, down_hbm), (up_whole, down_whole)

    def rows_of(owner, part=None):
        if part is None:
            return pl.ds(pl.multiple_of(owner * block, block), block)
        return pl.ds(pl.multiple_of(owner * block + part * piece, piece), piece)

    def columns_for(a):
        return pl.ds(pl.multiple_of((a % 2) * units, units), units)

    def z_copy(which, k, zk, part, sending):
        owner = sp if sending else 2 * zk + y
        return pltpu.make_async_remote_copy(
            src_ref=sources[which].at[pl.ds(part * piece, piece), columns_for(zk)],
            dst_ref=wholes[which].at[rows_of(owner, part)],
            send_sem=z_send.at[which, k, part],
            recv_sem=z_recv.at[which, k, part],
            device_id=(2 * zk + y, tp),
            device_id_type=MESH,
        )

    def y_copy(which, k, zk, part, sending):
        owner = 2 * zk + (y if sending else 1 - y)
        slot = wholes[which].at[rows_of(owner, part)]
        src = slot
        if isinstance(k, int) and k == 0:
            src = sources[which].at[pl.ds(part * piece, piece), columns_for(z)]
        return pltpu.make_async_remote_copy(
            src_ref=src,
            dst_ref=slot,
            send_sem=y_send.at[which, k, part],
            recv_sem=y_recv.at[which, k, part],
            device_id=(2 * z + 1 - y, tp),
            device_id_type=MESH,
        )

    def z_start(which, ks, first=0, last=None):
        for part, k in [(p, k) for p in range(pieces) for k in ks][first:last]:
            z_copy(which, k, xor(z, k), part, True).start()

    beyond = range(2, nz)
    many = pieces * len(beyond)
    early, before, quarter = (5 * many) // 8, (6 * many) // 8, many // 4

    def forward(which, k, zk, first=0, last=pieces):
        for part in range(first, last):
            z_copy(which, k, zk, part, False).wait_recv()
            y_copy(which, k, zk, part, True).start()

    def y_arrived(which, k, zk):
        for part in range(pieces):
            y_copy(which, k, zk, part, False).wait_recv()

    far = []
    for base in range(2, nz, 2):
        zb = xor(z, base)
        zf = flip(zb)
        far.append((base + inner, zb + inner * (zf - zb)))
        far.append((base + 1 - inner, zf + inner * (zb - zf)))
    near, distant = far[0::2], far[1::2]

    own = []
    for which in range(2):
        c = pltpu.make_async_copy(
            sources[which].at[:, columns_for(z)], wholes[which].at[rows_of(sp)], own_sem.at[which]
        )
        c.start()
        own.append(c)
    for part in range(pieces):
        y_copy(0, 0, z, part, True).start()
    z_start(0, (1,))

    @pl.when(inner == 1)
    def _():
        z_start(0, beyond, 0, early)

    gates = []
    for which, (source, target) in enumerate(((value_hbm, value_ref), (gate_hbm, gate_ref))):
        c = pltpu.make_async_copy(source, target, own_sem.at[2 + which])
        c.start()
        gates.append(c)

    def tp_at(a, b):
        return 2 * a + b

    def chan_core(i, c, sending):
        cols = pl.ds(c * kin, kin)
        slot = tp_at((x + nx - i) % nx, core if sending else 1 - core)
        return pltpu.make_async_remote_copy(
            src_ref=chan.at[slot, :, cols],
            dst_ref=chan.at[slot, :, cols],
            send_sem=chan_core_send.at[i, c],
            recv_sem=chan_core_recv.at[i, c],
            device_id=(sp, partner),
            device_id_type=MESH,
        )

    def chan_x(i, c, sending):
        cols = pl.ds(c * kin, kin)
        slot = tp if sending else tp_at((x + nx - i) % nx, core)
        return pltpu.make_async_remote_copy(
            src_ref=chan.at[slot, :, cols],
            dst_ref=chan.at[slot, :, cols],
            send_sem=chan_x_send.at[i - 1, c],
            recv_sem=chan_x_recv.at[i - 1, c],
            device_id=(sp, tp_at((x + i) % nx, core)),
            device_id_type=MESH,
        )

    def chan_forward(c):
        for i in range(1, nx):
            chan_x(i, c, False).wait_recv()
            chan_core(i, c, True).start()

    mixer_perm[...] = jnp.dot(
        perm_ref[...], mixer_ref[...], preferred_element_type=f32
    ).astype(bf16)
    highest = lax.Precision.HIGHEST
    step_size = lax.dot_general(
        perm_ref[...].astype(f32),
        jnp.exp(step_ref[...]),
        (((1,), (1,)), ((), ())),
        precision=highest,
        preferred_element_type=f32,
    )

    def iota(shape, axis):
        return lax.broadcasted_iota(jnp.int32, shape, axis)

    def ones_where(mask, dtype=f32):
        return jnp.where(mask, 1.0, 0.0).astype(dtype)

    def belongs(rows, columns, span, first):
        gap = iota((rows, columns), 1) + first - iota((rows, columns), 0) * span
        return ones_where((gap >= 0) & (gap < span))

    def tiled(size, copies):
        shape = (size, size * copies)
        hits = jnp.zeros(shape, f32)
        for i in range(copies):
            hits += ones_where(iota(shape, 1) - iota(shape, 0) == i * size)
        return hits

    over_states = tiled(states, bunch)
    agree = jnp.zeros((kin, lanes), f32)
    for i in range(bunch):
        r, l = iota((kin, lanes), 0) - i * each, iota((kin, lanes), 1) - i * states
        agree += ones_where((r >= 0) & (r < each) & (l >= 0) & (l < states))

    def wide_rate(table, c):
        spread = jnp.dot(table, over_states, precision=highest, preferred_element_type=f32)
        return jnp.sum(
            spread * belongs(groups, lanes, states, c * lanes), axis=0, keepdims=True
        )

    for c in range(chunks):
        cols = pl.ds(c * lanes, lanes)
        step_wide[...] = jnp.dot(
            step_size,
            belongs(groups, lanes, states, c * lanes),
            precision=highest,
            preferred_element_type=f32,
        )
        for i in range(2):
            matrix = jnp.dot(
                w_in_ref[i, c * kin : (c + 1) * kin, :].astype(bf16),
                over_states.astype(bf16),
                preferred_element_type=f32,
            )
            proj[:, i * lanes : (i + 1) * lanes] = jnp.dot(
                mixer_perm[:, c * kin : (c + 1) * kin],
                (matrix * agree).astype(bf16),
                preferred_element_type=f32,
            )
        rate_row = wide_rate(decay_ref[...], c)
        angle_row = wide_rate(angle_ref[...], c)
        modulus = rate_row * rate_row + angle_row * angle_row
        shape = (segments, lanes)
        rate = jnp.broadcast_to(rate_row, shape)
        half_angle = jnp.broadcast_to(angle_row * 0.5, shape)
        rate_n = jnp.broadcast_to(rate_row / modulus, shape)
        angle_n = jnp.broadcast_to(angle_row / modulus, shape)

        def one(j, state):
            pr, pi, sr, si = state
            rows = pl.ds(pl.multiple_of(j * segments, segments), segments)
            step = step_wide[rows, :]
            s, co = sine_cosine(half_angle * step)
            em = expm1_small(-rate * step)
            factor = 1.0 + em
            twice = 2.0 * s * s
            cos_r = 1.0 - twice
            dr = factor * cos_r
            di = factor * (2.0 * s * co)
            mr = em * cos_r - twice
            vr = di * angle_n - mr * rate_n
            vi = -di * rate_n - mr * angle_n
            a = proj[rows, 0:lanes]
            b = proj[rows, lanes : 2 * lanes]
            fr = vr * a - vi * b
            fi = vr * b + vi * a
            dre[rows, cols] = dr
            dim[rows, cols] = di
            fre[rows, cols] = fr
            fim[rows, cols] = fi
            return (
                dr * pr - di * pi,
                dr * pi + di * pr,
                dr * sr - di * si + fr,
                dr * si + di * sr + fi,
            )

        zero = jnp.zeros(shape, f32)
        last = lax.fori_loop(0, length, one, (zero + 1.0, zero, zero, zero), unroll=2)
        for i in range(4):
            ends[i, :, cols] = last[i]

    def link(earlier, later):
        return (
            later[0] * earlier[0] - later[1] * earlier[1] + later[2],
            later[0] * earlier[1] + later[1] * earlier[0] + later[3],
        )

    pr, pi, sr, si = (ends[i, 0:1, :] for i in range(4))
    for s in range(1, segments):
        qr, qi, tr, ti = (ends[i, s : s + 1, :] for i in range(4))
        pr, pi = qr * pr - qi * pi, qr * pi + qi * pr
        sr, si = link((sr, si), (qr, qi, tr, ti))
    for i, v in enumerate((pr, pi, sr, si)):
        carries[sp, i : i + 1, :] = v

    def carry_copy(i, sending):
        there = (sp + i) % n
        slot = sp if sending else (sp + n - i) % n
        return pltpu.make_async_remote_copy(
            src_ref=carries.at[slot],
            dst_ref=carries.at[slot],
            send_sem=carry_send.at[i - 1],
            recv_sem=carry_recv.at[i - 1],
            device_id=(there, tp),
            device_id_type=MESH,
        )

    for i in range(1, n):
        carry_copy(i, True).start()
    for i in range(1, n):
        carry_copy(i, False).wait_recv()
    cr = jnp.zeros_like(pr)
    ci = jnp.zeros_like(pr)
    for d in range(n - 1):
        nr, ni = link((cr, ci), tuple(carries[d, i : i + 1, :] for i in range(4)))
        cr = jnp.where(d < sp, nr, cr)
        ci = jnp.where(d < sp, ni, ci)
    for s in range(segments):
        entry[0, s : s + 1, :] = cr
        entry[1, s : s + 1, :] = ci
        cr, ci = link((cr, ci), tuple(ends[i, s : s + 1, :] for i in range(4)))

    @pl.when(inner == 1)
    def _():
        z_start(0, beyond, early)
        z_start(1, (1,))

    @pl.when(inner == 0)
    def _():
        z_start(0, beyond, 0, before)

    forward(0, 1, pair_z)
    half_way = pieces // 2
    for k, zk in near:
        forward(0, k, zk, 0, half_way)
    for part in range(pieces):
        y_copy(1, 0, z, part, True).start()

    for c in range(chunks):
        cols = pl.ds(c * lanes, lanes)

        def again(j, state):
            rows = pl.ds(pl.multiple_of(j * segments, segments), segments)
            dr, di = dre[rows, cols], dim[rows, cols]
            xr, xi = link(state, (dr, di, fre[rows, cols], fim[rows, cols]))
            proj[rows, 0:lanes] = xr
            proj[rows, lanes : 2 * lanes] = xi
            return xr, xi

        lax.fori_loop(0, length, again, (entry[0, :, cols], entry[1, :, cols]), unroll=4)
        ins = slice(c * kin, (c + 1) * kin)
        mech = jnp.zeros((tokens, kin), f32)
        for i in range(2):
            matrix = jnp.dot(
                w_out_ref[i, c * kin : (c + 1) * kin, :].astype(bf16),
                over_states.astype(bf16),
                preferred_element_type=f32,
            )
            mech += (1 - 2 * i) * lax.dot_general(
                proj[:, i * lanes : (i + 1) * lanes].astype(bf16),
                (matrix * agree).astype(bf16),
                (((1,), (1,)), ((), ())),
                preferred_element_type=f32,
            )
        mech = mech + skip_ref[0:1, ins] * mixer_perm[:, ins].astype(f32)
        mixed = jax.nn.gelu(mech).astype(bf16)
        chan[tp, :, ins] = jnp.dot(
            unperm_ref[...], mixed, preferred_element_type=f32
        ).astype(bf16)
        chan_core(0, c, True).start()
        for i in range(1, nx):
            chan_x(i, c, True).start()
        if c >= 2:
            chan_forward(c - 2)

    for c in range(max(chunks - 2, 0), chunks):
        chan_forward(c)
    for c in gates:
        c.wait()
    for c in range(chunks):
        for i in range(nx):
            chan_core(i, c, False).wait_recv()

    tile = 256

    @pl.loop(0, width // tile)
    def _(t):
        cols = pl.ds(pl.multiple_of(t * tile, tile), tile)
        v = jnp.zeros((tokens, tile), f32)
        g = jnp.zeros((tokens, tile), f32)
        for q in range(ntp):
            rows = slice(q * width, (q + 1) * width)
            v += jnp.dot(chan[q], value_ref[rows, cols], preferred_element_type=f32)
            g += jnp.dot(chan[q], gate_ref[rows, cols], preferred_element_type=f32)
        upd[0, tp, :, cols] = (resid_ref[:, cols].astype(f32) + v * jax.nn.sigmoid(g)).astype(bf16)

    def upd_z():
        return pltpu.make_async_remote_copy(
            src_ref=upd.at[0, tp],
            dst_ref=upd.at[1, tp],
            send_sem=upd_z_send.at[0],
            recv_sem=upd_z_recv.at[0],
            device_id=(pair, tp),
            device_id_type=MESH,
        )

    def upd_x(i, h, sending):
        slot = tp if sending else tp_at((x + nx - i) % nx, core)
        return pltpu.make_async_remote_copy(
            src_ref=upd.at[h, slot],
            dst_ref=upd.at[h, slot],
            send_sem=upd_x_send.at[i - 1, h],
            recv_sem=upd_x_recv.at[i - 1, h],
            device_id=(sp, tp_at((x + i) % nx, core)),
            device_id_type=MESH,
        )

    def upd_core(i, h, sending):
        slot = tp_at((x + nx - i) % nx, core if sending else 1 - core)
        return pltpu.make_async_remote_copy(
            src_ref=upd.at[h, slot],
            dst_ref=upd.at[h, slot],
            send_sem=upd_core_send.at[i, h],
            recv_sem=upd_core_recv.at[i, h],
            device_id=(sp, partner),
            device_id_type=MESH,
        )

    upd_z().start()
    for i in range(1, nx):
        upd_x(i, 0, True).start()
    upd_core(0, 0, True).start()

    @pl.when(inner == 0)
    def _():
        z_start(0, beyond, before)
        z_start(1, beyond)
        z_start(1, (1,))

    @pl.when(inner == 1)
    def _():
        z_start(1, beyond, 0, quarter)

    most = (3 * pieces) // 4
    for k, zk in distant:
        forward(0, k, zk, 0, most)
    for k, zk in near:
        forward(0, k, zk, half_way)
    for i in range(1, nx):
        upd_x(i, 0, False).wait_recv()
        upd_core(i, 0, True).start()
    upd_z().wait_recv()
    for i in range(1, nx):
        upd_x(i, 1, True).start()
    upd_core(0, 1, True).start()
    for k, zk in distant:
        forward(0, k, zk, most)

    @pl.when(inner == 0)
    def _():
        forward(1, 1, pair_z)

    def normalize(h):
        for i in range(nx):
            upd_core(i, h, False).wait_recv()
        total = jnp.zeros((tokens, 1), f32)
        for q in range(ntp):
            u = upd[h, q].astype(f32)
            total += jnp.sum(u * u, axis=1, keepdims=True)
        inv = lax.rsqrt(total * (1.0 / (width * ntp)) + rms_eps)
        for q in range(ntp):
            cols = slice(q * width, (q + 1) * width)
            normed[h * tokens : (h + 1) * tokens, cols] = (upd[h, q].astype(f32) * inv * gain_ref[0:1, cols]).astype(bf16)

    normalize(0)
    for i in range(1, nx):
        upd_x(i, 1, False).wait_recv()
        upd_core(i, 1, True).start()
    normalize(1)
    for c in own:
        c.wait()
    y_arrived(0, 0, z)
    y_arrived(0, 1, pair_z)
    for k, zk in far:
        y_arrived(0, k, zk)

    @pl.loop(0, units // tile)
    def _(t):
        cols = pl.ds(pl.multiple_of(t * tile, tile), tile)
        for h in range(2):
            some = slice(h * tokens, (h + 1) * tokens)
            r = jnp.dot(normed[some, :], up_whole[:, cols], preferred_element_type=f32)
            r = jnp.maximum(r, 0.0)
            hidden[some, cols] = (r * r).astype(bf16)

    def sum1(s):
        return pltpu.make_async_remote_copy(
            src_ref=out1.at[s],
            dst_ref=in1.at[s],
            send_sem=sum1_send.at[s],
            recv_sem=sum1_recv.at[s],
            device_id=(sp, partner),
            device_id_type=MESH,
        )

    def sum2(s):
        return pltpu.make_async_remote_copy(
            src_ref=out2.at[s],
            dst_ref=in2.at[s],
            send_sem=sum2_send.at[s],
            recv_sem=sum2_recv.at[s],
            device_id=(pair, tp),
            device_id_type=MESH,
        )

    def sum3(s, there, to):
        return pltpu.make_async_remote_copy(
            src_ref=out3.at[s],
            dst_ref=in3.at[s % per, there],
            send_sem=sum3_send.at[s],
            recv_sem=sum3_recv.at[s % per, there],
            device_id=(sp, to),
            device_id_type=MESH,
        )

    def core_of(s):
        return (s // per) % 2

    def x_of(s):
        return s // per // 2

    def stage1(s):
        rows = rows_of(s)

        @pl.loop(0, 2)
        def _(h):
            some = pl.ds(pl.multiple_of(h * tokens, tokens), tokens)
            keep[s, some, :] = lax.dot_general(
                hidden[some, :],
                down_whole[rows, :],
                (((1,), (1,)), ((), ())),
                preferred_element_type=f32,
            )

        @pl.when(core_of(s) != core)
        def _():
            out1[s] = keep[s].astype(bf16)
            sum1(s).start()

    def stage2(s):
        @pl.when(core_of(s) == core)
        def _():
            sum1(s).wait_recv()
            out2[s] = (keep[s, tokens:] + in1[s, tokens:].astype(f32)).astype(bf16)
            sum2(s).start()
            keep[s, :tokens] = keep[s, :tokens] + in1[s, :tokens].astype(f32)

    def stage3(s):
        @pl.when(core_of(s) == core)
        def _():
            sum2(s).wait_recv()
            total = keep[s, :tokens] + in2[s].astype(f32)

            @pl.when(x_of(s) == x)
            def _():
                keep[s, :tokens] = total

            @pl.when(x_of(s) != x)
            def _():
                out3[s] = total.astype(bf16)
                sum3(s, x, s // per).start()

    def step(k, zk, side):
        if side == 1:
            y_arrived(1, k, zk)
        s = 2 * zk + (y if side == 0 else 1 - y)
        stage1(s)
        if order and settled[-1] != len(order):
            stage2(order[-1])
        order.append(s)

    order, settled = [], [0]

    def settle(count):
        stage2(order[-1])
        settled.append(len(order))
        for s in order[count:]:
            stage3(s)

    for k, zk in distant:
        forward(1, k, zk, 0, half_way)
    for side in range(2):
        step(0, z, side)

    @pl.when(inner == 1)
    def _():
        z_start(1, beyond, quarter)

    for k, zk in distant:
        forward(1, k, zk, half_way)
    for k, zk in near:
        forward(1, k, zk, 0, pieces // 4)
    for k, zk in distant:
        for side in range(2):
            step(k, zk, side)

    @pl.when(inner == 1)
    def _():
        forward(1, 1, pair_z)

    for k, zk in near:
        forward(1, k, zk, pieces // 4, half_way)
    for side in range(2):
        step(1, pair_z, side)
    settle(0)
    for k, zk in near:
        forward(1, k, zk, half_way)
    done = len(order)
    for k, zk in near:
        for side in range(2):
            step(k, zk, side)
    settle(done)
    for j in range(per):
        s = tp * per + j
        cols = slice(j * block, (j + 1) * block)
        total = keep[s, :tokens]
        for i in range(1, nx):
            there = (x + i) % nx
            sum3(s, there, tp_at(there, core)).wait_recv()
            total += in3[j, there].astype(f32)
        out_ref[:, cols] = (upd[0, tp, :, cols].astype(f32) + total).astype(bf16)

    for which in range(2):
        for k in range(nz):
            for part in range(pieces):
                y_copy(which, k, xor(z, k), part, True).wait_send()
                if k > 0:
                    z_copy(which, k, xor(z, k), part, True).wait_send()
    for i in range(1, n):
        carry_copy(i, True).wait_send()
    for i in range(nx):
        for c in range(chunks):
            chan_core(i, c, True).wait_send()
            if i > 0:
                chan_x(i, c, True).wait_send()
        for h in range(2):
            upd_core(i, h, True).wait_send()
            if i > 0:
                upd_x(i, h, True).wait_send()
    upd_z().wait_send()
    for s in range(n):

        @pl.when(core_of(s) != core)
        def _():
            sum1(s).wait_send()

        @pl.when(core_of(s) == core)
        def _():
            sum2(s).wait_send()

        @pl.when((core_of(s) == core) & (x_of(s) != x))
        def _():
            sum3(s, x, s // per).wait_send()


def per_device(
    n,
    ntp,
    resid,
    mixer_in,
    log_step,
    decay_real,
    frequency,
    input_matrix,
    output_matrix,
    skip_gain,
    value_weight,
    gate_weight,
    norm_gain,
    up_weight,
    down_weight,
):
    tokens, width = mixer_in.shape
    groups, states = decay_real.shape
    each = width // groups
    bunch = min(128 // each, groups)
    chunks = groups // bunch
    lanes = bunch * states
    features, units = value_weight.shape[0], up_weight.shape[1] // 2
    block = up_weight.shape[0]
    length = tokens // segments
    row = np.arange(tokens)
    perm = (row[None, :] == ((row % segments) * length + row // segments)[:, None]).astype(np.float32)
    nz, nx, per, pieces = n // 2, ntp // 2, n // ntp, 4
    total = groups * states
    dma = pltpu.SemaphoreType.DMA
    vmem = pl.BlockSpec(memory_space=pltpu.VMEM)
    hbm = pl.BlockSpec(memory_space=pl.ANY)
    return pl.pallas_call(
        functools.partial(kernel, n, ntp),
        out_shape=jax.ShapeDtypeStruct((tokens, width), bf16),
        in_specs=[vmem] * 8 + [hbm] * 2 + [vmem] + [hbm] * 2 + [vmem] * 2,
        out_specs=vmem,
        scratch_shapes=[
            pltpu.VMEM((features, units), bf16),
            pltpu.VMEM((features, units), bf16),
            pltpu.VMEM((features, width), bf16),
            pltpu.VMEM((features, width), bf16),
            pltpu.VMEM((tokens, total), f32),
            pltpu.VMEM((tokens, total), f32),
            pltpu.VMEM((tokens, total), f32),
            pltpu.VMEM((tokens, total), f32),
            pltpu.VMEM((tokens, lanes), f32),
            pltpu.VMEM((tokens, 2 * lanes), f32),
            pltpu.VMEM((4, segments, total), f32),
            pltpu.VMEM((n, 4, total), f32),
            pltpu.VMEM((2, segments, total), f32),
            pltpu.VMEM((tokens, width), bf16),
            pltpu.VMEM((ntp, tokens, width), bf16),
            pltpu.VMEM((2, ntp, tokens, width), bf16),
            pltpu.VMEM((2 * tokens, features), bf16),
            pltpu.VMEM((2 * tokens, units), bf16),
            pltpu.VMEM((n, 2 * tokens, block), f32),
            pltpu.VMEM((n, 2 * tokens, block), bf16),
            pltpu.VMEM((n, 2 * tokens, block), bf16),
            pltpu.VMEM((n, tokens, block), bf16),
            pltpu.VMEM((n, tokens, block), bf16),
            pltpu.VMEM((n, tokens, block), bf16),
            pltpu.VMEM((per, nx, tokens, block), bf16),
            dma((4,)),
            dma((2, nz, pieces)),
            dma((2, nz, pieces)),
            dma((2, nz, pieces)),
            dma((2, nz, pieces)),
            dma((n - 1,)),
            dma((n - 1,)),
            dma((nx, chunks)),
            dma((nx, chunks)),
            dma((max(nx - 1, 1), chunks)),
            dma((max(nx - 1, 1), chunks)),
            dma((1,)),
            dma((1,)),
            dma((nx, 2)),
            dma((nx, 2)),
            dma((max(nx - 1, 1), 2)),
            dma((max(nx - 1, 1), 2)),
            dma((n,)),
            dma((n,)),
            dma((n,)),
            dma((n,)),
            dma((n,)),
            dma((per, nx)),
        ],
        compiler_params=pltpu.CompilerParams(
            collective_id=0, has_side_effects=True, vmem_limit_bytes=64 * 1024 * 1024 - 65536
        ),
    )(
        resid,
        mixer_in,
        log_step.T,
        decay_real,
        frequency,
        jnp.transpose(input_matrix, (0, 1, 3, 2)).reshape(2, width, states),
        output_matrix.reshape(2, width, states),
        skip_gain.reshape(1, width),
        value_weight,
        gate_weight,
        norm_gain.reshape(1, features),
        up_weight,
        down_weight,
        jnp.asarray(perm, bf16),
        jnp.asarray(perm.T, bf16),
    )


def solution(mesh):
    in_specs = (
        P("sp", "tp"),
        P("sp", "tp"),
        P("sp", "tp"),
        P("tp", None),
        P("tp", None),
        P(None, "tp", None, None),
        P(None, "tp", None, None),
        P("tp"),
        P(None, "tp"),
        P(None, "tp"),
        P(),
        P("sp", "tp"),
        P("sp", "tp"),
    )
    body = functools.partial(per_device, mesh.shape["sp"], mesh.shape["tp"])
    return jax.shard_map(
        body, mesh=mesh, in_specs=in_specs, out_specs=P("sp", "tp"), check_vma=False
    )
```

```python
import functools

import jax
import jax.numpy as jnp
import numpy as np
from jax import lax
from jax.experimental import pallas as pl
from jax.experimental.pallas import tpu as pltpu
from jax.sharding import PartitionSpec as P

rms_eps = 1e-06
segments = 8
MESH = pl.DeviceIdType.MESH
f32, bf16 = jnp.float32, jnp.bfloat16


def sine_cosine(x):
    y = x * x
    s = 1.0 + y * (-1 / 6 + y * (1 / 120 + y * (-1 / 5040 + y * (1 / 362880 + y * (-1 / 39916800)))))
    c = 1.0 + y * (
        -0.5
        + y * (1 / 24 + y * (-1 / 720 + y * (1 / 40320 + y * (-1 / 3628800 + y * (1 / 479001600)))))
    )
    return x * s, c


def expm1_small(y):
    return y * (
        1.0
        + y * (1 / 2 + y * (1 / 6 + y * (1 / 24 + y * (1 / 120 + y * (1 / 720 + y * (1 / 5040))))))
    )


def kernel(
    n,
    ntp,
    resid_ref,
    mixer_ref,
    step_ref,
    decay_ref,
    angle_ref,
    w_in_ref,
    w_out_ref,
    skip_ref,
    value_hbm,
    gate_hbm,
    gain_ref,
    up_hbm,
    down_hbm,
    perm_ref,
    unperm_ref,
    out_ref,
    up_whole,
    down_whole,
    value_ref,
    gate_ref,
    dre,
    dim,
    fre,
    fim,
    step_wide,
    proj,
    ends,
    carries,
    mate,
    prefix,
    entry,
    mixer_perm,
    chan,
    upd,
    normed,
    hidden,
    keep,
    out1,
    in1,
    out2,
    in2,
    out3,
    in3,
    own_sem,
    z_send,
    z_recv,
    y_send,
    y_recv,
    carry_send,
    carry_recv,
    chan_core_send,
    chan_core_recv,
    chan_x_send,
    chan_x_recv,
    upd_z_send,
    upd_z_recv,
    upd_core_send,
    upd_core_recv,
    upd_x_send,
    upd_x_recv,
    sum1_send,
    sum1_recv,
    sum2_send,
    sum2_recv,
    sum3_send,
    sum3_recv,
):
    sp = lax.axis_index("sp")
    tp = lax.axis_index("tp")
    tokens, width = mixer_ref.shape
    block = up_hbm.shape[0]
    units = up_whole.shape[1]
    groups, states = decay_ref.shape
    each = width // groups
    bunch = min(128 // each, groups)
    chunks = groups // bunch
    lanes, kin = bunch * states, bunch * each
    length = tokens // segments
    pieces = z_recv.shape[2]
    piece = block // pieces
    nz, nx, per = n // 2, ntp // 2, n // ntp
    z, y = sp // 2, sp % 2
    x, core = tp // 2, tp % 2
    partner = tp + 1 - 2 * core

    def xor(a, k):
        total = 0
        bit = 1
        while bit < nz:
            digit = (a // bit) % 2
            total = total + bit * (1 - digit if k & bit else digit)
            bit *= 2
        return total

    def flip(a):
        return a + 1 - 2 * (a % 2)

    pair_z = flip(z)
    pair = 2 * pair_z + y
    inner = ((z + 1) // 2) % 2

    barrier = pltpu.get_barrier_semaphore()
    for i in range(1, n):
        pl.semaphore_signal(barrier, inc=1, device_id=((sp + i) % n, tp), device_id_type=MESH)
    for i in range(1, ntp):
        pl.semaphore_signal(barrier, inc=1, device_id=(sp, (tp + i) % ntp), device_id_type=MESH)
    pl.semaphore_wait(barrier, n - 1 + ntp - 1)

    sources, wholes = (up_hbm, down_hbm), (up_whole, down_whole)

    def rows_of(owner, part=None):
        if part is None:
            return pl.ds(pl.multiple_of(owner * block, block), block)
        return pl.ds(pl.multiple_of(owner * block + part * piece, piece), piece)

    def columns_for(a):
        return pl.ds(pl.multiple_of((a % 2) * units, units), units)

    def z_copy(which, k, zk, part, sending):
        owner = sp if sending else 2 * zk + y
        return pltpu.make_async_remote_copy(
            src_ref=sources[which].at[pl.ds(part * piece, piece), columns_for(zk)],
            dst_ref=wholes[which].at[rows_of(owner, part)],
            send_sem=z_send.at[which, k],
            recv_sem=z_recv.at[which, k, part],
            device_id=(2 * zk + y, tp),
            device_id_type=MESH,
        )

    def y_copy(which, k, zk, part, sending):
        owner = 2 * zk + (y if sending else 1 - y)
        slot = wholes[which].at[rows_of(owner, part)]
        src = slot
        if isinstance(k, int) and k == 0:
            src = sources[which].at[pl.ds(part * piece, piece), columns_for(z)]
        return pltpu.make_async_remote_copy(
            src_ref=src,
            dst_ref=slot,
            send_sem=y_send.at[which, k],
            recv_sem=y_recv.at[which, k, part],
            device_id=(2 * z + 1 - y, tp),
            device_id_type=MESH,
        )

    def z_start(which, ks, first=0, last=None):
        for part, k in [(p, k) for p in range(pieces) for k in ks][first:last]:
            z_copy(which, k, xor(z, k), part, True).start()

    beyond = range(2, nz)
    many = pieces * len(beyond)
    early, before, quarter = (5 * many) // 8, (6 * many) // 8, many // 4

    def forward(which, k, zk, first=0, last=pieces):
        for part in range(first, last):
            z_copy(which, k, zk, part, False).wait_recv()
            y_copy(which, k, zk, part, True).start()

    def y_arrived(which, k, zk):
        for part in range(pieces):
            y_copy(which, k, zk, part, False).wait_recv()

    far = []
    for base in range(2, nz, 2):
        zb = xor(z, base)
        zf = flip(zb)
        far.append((base + inner, zb + inner * (zf - zb)))
        far.append((base + 1 - inner, zf + inner * (zb - zf)))
    near, distant = far[0::2], far[1::2]

    own = []
    for which in range(2):
        c = pltpu.make_async_copy(
            sources[which].at[:, columns_for(z)], wholes[which].at[rows_of(sp)], own_sem.at[which]
        )
        c.start()
        own.append(c)
    for part in range(pieces):
        y_copy(0, 0, z, part, True).start()
    z_start(0, (1,))

    @pl.when(inner == 1)
    def _():
        z_start(0, beyond, 0, early)

    gates = []
    for which, (source, target) in enumerate(((value_hbm, value_ref), (gate_hbm, gate_ref))):
        c = pltpu.make_async_copy(source, target, own_sem.at[2 + which])
        c.start()
        gates.append(c)

    def tp_at(a, b):
        return 2 * a + b

    def chan_core(i, c, sending):
        cols = pl.ds(c * kin, kin)
        slot = tp_at((x + nx - i) % nx, core if sending else 1 - core)
        return pltpu.make_async_remote_copy(
            src_ref=chan.at[slot, :, cols],
            dst_ref=chan.at[slot, :, cols],
            send_sem=chan_core_send.at[i, c],
            recv_sem=chan_core_recv.at[i, c],
            device_id=(sp, partner),
            device_id_type=MESH,
        )

    def chan_x(i, c, sending):
        cols = pl.ds(c * kin, kin)
        slot = tp if sending else tp_at((x + nx - i) % nx, core)
        return pltpu.make_async_remote_copy(
            src_ref=chan.at[slot, :, cols],
            dst_ref=chan.at[slot, :, cols],
            send_sem=chan_x_send.at[i - 1, c],
            recv_sem=chan_x_recv.at[i - 1, c],
            device_id=(sp, tp_at((x + i) % nx, core)),
            device_id_type=MESH,
        )

    def chan_forward(c):
        for i in range(1, nx):
            chan_x(i, c, False).wait_recv()
            chan_core(i, c, True).start()

    mixer_perm[...] = jnp.dot(
        perm_ref[...], mixer_ref[...], preferred_element_type=f32
    ).astype(bf16)
    highest = lax.Precision.HIGHEST
    step_size = lax.dot_general(
        perm_ref[...].astype(f32),
        jnp.exp(step_ref[...]),
        (((1,), (1,)), ((), ())),
        precision=highest,
        preferred_element_type=f32,
    )

    def iota(shape, axis):
        return lax.broadcasted_iota(jnp.int32, shape, axis)

    def ones_where(mask, dtype=f32):
        return jnp.where(mask, 1.0, 0.0).astype(dtype)

    def belongs(rows, columns, span, first):
        gap = iota((rows, columns), 1) + first - iota((rows, columns), 0) * span
        return ones_where((gap >= 0) & (gap < span))

    def tiled(size, copies):
        shape = (size, size * copies)
        hits = jnp.zeros(shape, f32)
        for i in range(copies):
            hits += ones_where(iota(shape, 1) - iota(shape, 0) == i * size)
        return hits

    over_states = tiled(states, bunch)
    agree = jnp.zeros((kin, lanes), f32)
    for i in range(bunch):
        r, l = iota((kin, lanes), 0) - i * each, iota((kin, lanes), 1) - i * states
        agree += ones_where((r >= 0) & (r < each) & (l >= 0) & (l < states))

    def wide_rate(table, c):
        spread = jnp.dot(table, over_states, precision=highest, preferred_element_type=f32)
        return jnp.sum(
            spread * belongs(groups, lanes, states, c * lanes), axis=0, keepdims=True
        )

    for c in range(chunks):
        cols = pl.ds(c * lanes, lanes)
        step_wide[...] = jnp.dot(
            step_size,
            belongs(groups, lanes, states, c * lanes),
            precision=highest,
            preferred_element_type=f32,
        )
        for i in range(2):
            matrix = jnp.dot(
                w_in_ref[i, c * kin : (c + 1) * kin, :].astype(bf16),
                over_states.astype(bf16),
                preferred_element_type=f32,
            )
            proj[:, i * lanes : (i + 1) * lanes] = jnp.dot(
                mixer_perm[:, c * kin : (c + 1) * kin],
                (matrix * agree).astype(bf16),
                preferred_element_type=f32,
            )
        rate_row = wide_rate(decay_ref[...], c)
        angle_row = wide_rate(angle_ref[...], c)
        modulus = rate_row * rate_row + angle_row * angle_row
        shape = (segments, lanes)
        rate = jnp.broadcast_to(rate_row, shape)
        half_angle = jnp.broadcast_to(angle_row * 0.5, shape)
        rate_n = jnp.broadcast_to(rate_row / modulus, shape)
        angle_n = jnp.broadcast_to(angle_row / modulus, shape)

        def one(j, state):
            pr, pi, sr, si = state
            rows = pl.ds(pl.multiple_of(j * segments, segments), segments)
            step = step_wide[rows, :]
            s, co = sine_cosine(half_angle * step)
            em = expm1_small(-rate * step)
            factor = 1.0 + em
            twice = 2.0 * s * s
            cos_r = 1.0 - twice
            dr = factor * cos_r
            di = factor * (2.0 * s * co)
            mr = em * cos_r - twice
            vr = di * angle_n - mr * rate_n
            vi = -di * rate_n - mr * angle_n
            a = proj[rows, 0:lanes]
            b = proj[rows, lanes : 2 * lanes]
            fr = vr * a - vi * b
            fi = vr * b + vi * a
            dre[rows, cols] = dr
            dim[rows, cols] = di
            fre[rows, cols] = fr
            fim[rows, cols] = fi
            return (
                dr * pr - di * pi,
                dr * pi + di * pr,
                dr * sr - di * si + fr,
                dr * si + di * sr + fi,
            )

        zero = jnp.zeros(shape, f32)
        last = lax.fori_loop(0, length, one, (zero + 1.0, zero, zero, zero), unroll=2)
        for i in range(4):
            ends[i, :, cols] = last[i]

    def link(earlier, later):
        return (
            later[0] * earlier[0] - later[1] * earlier[1] + later[2],
            later[0] * earlier[1] + later[1] * earlier[0] + later[3],
        )

    def chain(first, second):
        fr, fi, ur, ui = first
        qr, qi, tr, ti = second
        vr, vi = link((ur, ui), second)
        return qr * fr - qi * fi, qr * fi + qi * fr, vr, vi

    def four(ref, *at):
        return tuple(ref[(*at, slice(i, i + 1), slice(None))] for i in range(4))

    whole_run = tuple(ends[i, 0:1, :] for i in range(4))
    for s in range(1, segments):
        whole_run = chain(whole_run, tuple(ends[i, s : s + 1, :] for i in range(4)))
    for i, v in enumerate(whole_run):
        mate[y, i : i + 1, :] = v

    def mate_copy(sending):
        slot = y if sending else 1 - y
        return pltpu.make_async_remote_copy(
            src_ref=mate.at[slot],
            dst_ref=mate.at[slot],
            send_sem=carry_send.at[0],
            recv_sem=carry_recv.at[0],
            device_id=(2 * z + 1 - y, tp),
            device_id_type=MESH,
        )

    def carry_copy(i, sending):
        slot = z if sending else (z + nz - i) % nz
        return pltpu.make_async_remote_copy(
            src_ref=carries.at[slot],
            dst_ref=carries.at[slot],
            send_sem=carry_send.at[i],
            recv_sem=carry_recv.at[i],
            device_id=(2 * ((z + i) % nz) + y, tp),
            device_id_type=MESH,
        )

    upper = z // (nz // 2)

    def second_sends():
        @pl.when(inner == 1)
        def _():
            z_start(0, beyond, early)

        @pl.when(inner == 0)
        def _():
            z_start(0, beyond, 0, before)

    pl.when(upper == 1)(second_sends)
    mate_copy(True).start()
    for part in range(pieces):
        y_copy(1, 0, z, part, True).start()
    mate_copy(False).wait_recv()
    for i, v in enumerate(chain(four(mate, 0), four(mate, 1))):
        carries[z, i : i + 1, :] = v
    for i in range(1, nz):

        @pl.when(z + i < nz)
        def _():
            carry_copy(i, True).start()

    prefix[...] = jnp.zeros_like(prefix)

    def extend(run):
        for i, v in enumerate(link((prefix[0:1, :], prefix[1:2, :]), run)):
            prefix[i : i + 1, :] = v

    for i in range(1, nz):

        @pl.when(z >= i)
        def _():
            carry_copy(i, False).wait_recv()

    for i in range(1, nz):

        @pl.when(z + i < nz)
        def _():
            carry_copy(i, True).wait_send()

    pl.when(upper == 0)(second_sends)

    for d in range(nz - 1):

        @pl.when(d < z)
        def _():
            extend(four(carries, d))

    @pl.when(y == 1)
    def _():
        extend(four(mate, 0))

    cr, ci = prefix[0:1, :], prefix[1:2, :]
    for s in range(segments):
        entry[0, s : s + 1, :] = cr
        entry[1, s : s + 1, :] = ci
        cr, ci = link((cr, ci), tuple(ends[i, s : s + 1, :] for i in range(4)))
    forward(0, 1, pair_z)
    half_way = pieces // 2
    for k, zk in near:
        forward(0, k, zk, 0, half_way)

    for c in range(chunks):
        cols = pl.ds(c * lanes, lanes)

        def again(j, state):
            rows = pl.ds(pl.multiple_of(j * segments, segments), segments)
            dr, di = dre[rows, cols], dim[rows, cols]
            xr, xi = link(state, (dr, di, fre[rows, cols], fim[rows, cols]))
            proj[rows, 0:lanes] = xr
            proj[rows, lanes : 2 * lanes] = xi
            return xr, xi

        lax.fori_loop(0, length, again, (entry[0, :, cols], entry[1, :, cols]), unroll=4)
        ins = slice(c * kin, (c + 1) * kin)
        mech = jnp.zeros((tokens, kin), f32)
        for i in range(2):
            matrix = jnp.dot(
                w_out_ref[i, c * kin : (c + 1) * kin, :].astype(bf16),
                over_states.astype(bf16),
                preferred_element_type=f32,
            )
            mech += (1 - 2 * i) * lax.dot_general(
                proj[:, i * lanes : (i + 1) * lanes].astype(bf16),
                (matrix * agree).astype(bf16),
                (((1,), (1,)), ((), ())),
                preferred_element_type=f32,
            )
        mech = mech + skip_ref[0:1, ins] * mixer_perm[:, ins].astype(f32)
        mixed = jax.nn.gelu(mech).astype(bf16)
        chan[tp, :, ins] = jnp.dot(
            unperm_ref[...], mixed, preferred_element_type=f32
        ).astype(bf16)
        chan_core(0, c, True).start()
        for i in range(1, nx):
            chan_x(i, c, True).start()
        if c >= 2:
            chan_forward(c - 2)

    for c in range(max(chunks - 2, 0), chunks):
        chan_forward(c)
    for c in gates:
        c.wait()
    for c in range(chunks):
        for i in range(nx):
            chan_core(i, c, False).wait_recv()

    tile = 256

    @pl.loop(0, width // tile)
    def _(t):
        cols = pl.ds(pl.multiple_of(t * tile, tile), tile)
        v = jnp.zeros((tokens, tile), f32)
        g = jnp.zeros((tokens, tile), f32)
        for q in range(ntp):
            rows = slice(q * width, (q + 1) * width)
            v += jnp.dot(chan[q], value_ref[rows, cols], preferred_element_type=f32)
            g += jnp.dot(chan[q], gate_ref[rows, cols], preferred_element_type=f32)
        upd[0, tp, :, cols] = (resid_ref[:, cols].astype(f32) + v * jax.nn.sigmoid(g)).astype(bf16)

    def upd_z():
        return pltpu.make_async_remote_copy(
            src_ref=upd.at[0, tp],
            dst_ref=upd.at[1, tp],
            send_sem=upd_z_send.at[0],
            recv_sem=upd_z_recv.at[0],
            device_id=(pair, tp),
            device_id_type=MESH,
        )

    def upd_x(i, h, sending):
        slot = tp if sending else tp_at((x + nx - i) % nx, core)
        return pltpu.make_async_remote_copy(
            src_ref=upd.at[h, slot],
            dst_ref=upd.at[h, slot],
            send_sem=upd_x_send.at[i - 1, h],
            recv_sem=upd_x_recv.at[i - 1, h],
            device_id=(sp, tp_at((x + i) % nx, core)),
            device_id_type=MESH,
        )

    def upd_core(i, h, sending):
        slot = tp_at((x + nx - i) % nx, core if sending else 1 - core)
        return pltpu.make_async_remote_copy(
            src_ref=upd.at[h, slot],
            dst_ref=upd.at[h, slot],
            send_sem=upd_core_send.at[i, h],
            recv_sem=upd_core_recv.at[i, h],
            device_id=(sp, partner),
            device_id_type=MESH,
        )

    upd_z().start()
    for i in range(1, nx):
        upd_x(i, 0, True).start()
    upd_core(0, 0, True).start()

    @pl.when(inner == 0)
    def _():
        z_start(0, beyond, before)
        for k in beyond:
            z_start(1, (k,))
        z_start(1, (1,))

    @pl.when(inner == 1)
    def _():
        z_start(1, beyond, 0, quarter)
        z_start(1, (1,))

    most = (3 * pieces) // 4
    for k, zk in distant:
        forward(0, k, zk, 0, most)
    for k, zk in near:
        forward(0, k, zk, half_way)
    for i in range(1, nx):
        upd_x(i, 0, False).wait_recv()
        upd_core(i, 0, True).start()
    upd_z().wait_recv()
    for i in range(1, nx):
        upd_x(i, 1, True).start()
    upd_core(0, 1, True).start()
    for k, zk in distant:
        forward(0, k, zk, most)

    def normalize(h):
        for i in range(nx):
            upd_core(i, h, False).wait_recv()
        total = jnp.zeros((tokens, 1), f32)
        for q in range(ntp):
            u = upd[h, q].astype(f32)
            total += jnp.sum(u * u, axis=1, keepdims=True)
        inv = lax.rsqrt(total * (1.0 / (width * ntp)) + rms_eps)
        for q in range(ntp):
            cols = slice(q * width, (q + 1) * width)
            normed[h * tokens : (h + 1) * tokens, cols] = (upd[h, q].astype(f32) * inv * gain_ref[0:1, cols]).astype(bf16)

    normalize(0)
    for i in range(1, nx):
        upd_x(i, 1, False).wait_recv()
        upd_core(i, 1, True).start()
    normalize(1)

    @pl.when(inner == 0)
    def _():
        forward(1, 1, pair_z)

    for c in own:
        c.wait()
    y_arrived(0, 0, z)
    y_arrived(0, 1, pair_z)
    for k, zk in far:
        y_arrived(0, k, zk)

    @pl.loop(0, units // tile)
    def _(t):
        cols = pl.ds(pl.multiple_of(t * tile, tile), tile)
        for h in range(2):
            some = slice(h * tokens, (h + 1) * tokens)
            r = jnp.dot(normed[some, :], up_whole[:, cols], preferred_element_type=f32)
            r = jnp.maximum(r, 0.0)
            hidden[some, cols] = (r * r).astype(bf16)

    def sum1(s):
        return pltpu.make_async_remote_copy(
            src_ref=out1.at[s],
            dst_ref=in1.at[s],
            send_sem=sum1_send.at[s],
            recv_sem=sum1_recv.at[s],
            device_id=(sp, partner),
            device_id_type=MESH,
        )

    def sum2(s):
        return pltpu.make_async_remote_copy(
            src_ref=out2.at[s],
            dst_ref=in2.at[s],
            send_sem=sum2_send.at[s],
            recv_sem=sum2_recv.at[s],
            device_id=(pair, tp),
            device_id_type=MESH,
        )

    def sum3(s, there, to):
        return pltpu.make_async_remote_copy(
            src_ref=out3.at[s],
            dst_ref=in3.at[s % per, there],
            send_sem=sum3_send.at[s],
            recv_sem=sum3_recv.at[s % per, there],
            device_id=(sp, to),
            device_id_type=MESH,
        )

    def core_of(s):
        return (s // per) % 2

    def x_of(s):
        return s // per // 2

    def stage1(s):
        rows = rows_of(s)

        @pl.loop(0, 2)
        def _(h):
            some = pl.ds(pl.multiple_of(h * tokens, tokens), tokens)
            keep[s, some, :] = lax.dot_general(
                hidden[some, :],
                down_whole[rows, :],
                (((1,), (1,)), ((), ())),
                preferred_element_type=f32,
            )

        @pl.when(core_of(s) != core)
        def _():
            out1[s] = keep[s].astype(bf16)
            sum1(s).start()

    def stage2(s):
        @pl.when(core_of(s) == core)
        def _():
            sum1(s).wait_recv()
            out2[s] = (keep[s, tokens:] + in1[s, tokens:].astype(f32)).astype(bf16)
            sum2(s).start()
            keep[s, :tokens] = keep[s, :tokens] + in1[s, :tokens].astype(f32)

    def stage3(s):
        @pl.when(core_of(s) == core)
        def _():
            sum2(s).wait_recv()
            total = keep[s, :tokens] + in2[s].astype(f32)

            @pl.when(x_of(s) == x)
            def _():
                keep[s, :tokens] = total

            @pl.when(x_of(s) != x)
            def _():
                out3[s] = total.astype(bf16)
                sum3(s, x, s // per).start()

    def step(k, zk, side, eager=False):
        if side == 1:
            y_arrived(1, k, zk)
        s = 2 * zk + (y if side == 0 else 1 - y)
        stage1(s)
        if waiting:
            stage2(waiting.pop())
        if eager:
            stage2(s)
        else:
            waiting.append(s)
        order.append(s)

    order, waiting = [], []

    def weights_sent(which):
        slot = wholes[which].at[rows_of(sp)]
        for k in range(nz):
            for sem in (y_send, z_send)[: 1 + (k > 0)]:
                pltpu.make_async_remote_copy(
                    src_ref=slot,
                    dst_ref=slot,
                    send_sem=sem.at[which, k],
                    recv_sem=z_recv.at[which, k, 0],
                    device_id=(2 * z + 1 - y, tp),
                    device_id_type=MESH,
                ).wait_send()

    def first_sent():
        weights_sent(0)
        mate_copy(True).wait_send()
        for i in range(nx):
            for c in range(chunks):
                chan_core(i, c, True).wait_send()
                if i > 0:
                    chan_x(i, c, True).wait_send()
            for h in range(2):
                upd_core(i, h, True).wait_send()
                if i > 0:
                    upd_x(i, h, True).wait_send()
        upd_z().wait_send()

    for k, zk in distant:
        forward(1, k, zk, 0, half_way)
    for side in range(2):
        step(0, z, side)

    @pl.when(inner == 1)
    def _():
        z_start(1, beyond, quarter)

    for k, zk in distant:
        forward(1, k, zk, half_way)

    for k, zk in near:
        forward(1, k, zk, 0, pieces // 4)
    for k, zk in distant:
        for side in range(2):
            step(k, zk, side)
    stage2(waiting.pop())

    @pl.when(inner == 1)
    def _():
        forward(1, 1, pair_z)

    for k, zk in near:
        forward(1, k, zk, pieces // 4, half_way)
    for s in order[2:]:
        stage3(s)
    for side in range(2):
        step(1, pair_z, side)
    stage2(waiting.pop())
    first_sent()
    for k, zk in near:
        forward(1, k, zk, half_way, most)
    for k, zk in near:
        forward(1, k, zk, most)
    remaining = order[:2] + order[-2:]
    done = len(order)
    for side in range(2):
        for k, zk in near:
            step(k, zk, side, True)
        if side == 0:
            for s in remaining:
                stage3(s)
    for s in order[done:]:
        stage3(s)
    for j in range(per):
        s = tp * per + j
        cols = slice(j * block, (j + 1) * block)
        total = keep[s, :tokens]
        for i in range(1, nx):
            there = (x + i) % nx
            sum3(s, there, tp_at(there, core)).wait_recv()
            total += in3[j, there].astype(f32)
        out_ref[:, cols] = (upd[0, tp, :, cols].astype(f32) + total).astype(bf16)

    weights_sent(1)
    for s in range(n):

        @pl.when(core_of(s) != core)
        def _():
            sum1(s).wait_send()

        @pl.when(core_of(s) == core)
        def _():
            sum2(s).wait_send()

        @pl.when((core_of(s) == core) & (x_of(s) != x))
        def _():
            sum3(s, x, s // per).wait_send()


def per_device(
    n,
    ntp,
    resid,
    mixer_in,
    log_step,
    decay_real,
    frequency,
    input_matrix,
    output_matrix,
    skip_gain,
    value_weight,
    gate_weight,
    norm_gain,
    up_weight,
    down_weight,
):
    tokens, width = mixer_in.shape
    groups, states = decay_real.shape
    each = width // groups
    bunch = min(128 // each, groups)
    chunks = groups // bunch
    lanes = bunch * states
    features, units = value_weight.shape[0], up_weight.shape[1] // 2
    block = up_weight.shape[0]
    length = tokens // segments
    row = np.arange(tokens)
    perm = (row[None, :] == ((row % segments) * length + row // segments)[:, None]).astype(np.float32)
    nz, nx, per, pieces = n // 2, ntp // 2, n // ntp, 4
    total = groups * states
    dma = pltpu.SemaphoreType.DMA
    vmem = pl.BlockSpec(memory_space=pltpu.VMEM)
    hbm = pl.BlockSpec(memory_space=pl.ANY)
    return pl.pallas_call(
        functools.partial(kernel, n, ntp),
        out_shape=jax.ShapeDtypeStruct((tokens, width), bf16),
        in_specs=[vmem] * 8 + [hbm] * 2 + [vmem] + [hbm] * 2 + [vmem] * 2,
        out_specs=vmem,
        scratch_shapes=[
            pltpu.VMEM((features, units), bf16),
            pltpu.VMEM((features, units), bf16),
            pltpu.VMEM((features, width), bf16),
            pltpu.VMEM((features, width), bf16),
            pltpu.VMEM((tokens, total), f32),
            pltpu.VMEM((tokens, total), f32),
            pltpu.VMEM((tokens, total), f32),
            pltpu.VMEM((tokens, total), f32),
            pltpu.VMEM((tokens, lanes), f32),
            pltpu.VMEM((tokens, 2 * lanes), f32),
            pltpu.VMEM((4, segments, total), f32),
            pltpu.VMEM((nz, 4, total), f32),
            pltpu.VMEM((2, 4, total), f32),
            pltpu.VMEM((2, total), f32),
            pltpu.VMEM((2, segments, total), f32),
            pltpu.VMEM((tokens, width), bf16),
            pltpu.VMEM((ntp, tokens, width), bf16),
            pltpu.VMEM((2, ntp, tokens, width), bf16),
            pltpu.VMEM((2 * tokens, features), bf16),
            pltpu.VMEM((2 * tokens, units), bf16),
            pltpu.VMEM((n, 2 * tokens, block), f32),
            pltpu.VMEM((n, 2 * tokens, block), bf16),
            pltpu.VMEM((n, 2 * tokens, block), bf16),
            pltpu.VMEM((n, tokens, block), bf16),
            pltpu.VMEM((n, tokens, block), bf16),
            pltpu.VMEM((n, tokens, block), bf16),
            pltpu.VMEM((per, nx, tokens, block), bf16),
            dma((4,)),
            dma((2, nz)),
            dma((2, nz, pieces)),
            dma((2, nz)),
            dma((2, nz, pieces)),
            dma((nz,)),
            dma((nz,)),
            dma((nx, chunks)),
            dma((nx, chunks)),
            dma((max(nx - 1, 1), chunks)),
            dma((max(nx - 1, 1), chunks)),
            dma((1,)),
            dma((1,)),
            dma((nx, 2)),
            dma((nx, 2)),
            dma((max(nx - 1, 1), 2)),
            dma((max(nx - 1, 1), 2)),
            dma((n,)),
            dma((n,)),
            dma((n,)),
            dma((n,)),
            dma((n,)),
            dma((per, nx)),
        ],
        compiler_params=pltpu.CompilerParams(
            collective_id=0, has_side_effects=True, vmem_limit_bytes=64 * 1024 * 1024 - 65536
        ),
    )(
        resid,
        mixer_in,
        log_step.T,
        decay_real,
        frequency,
        jnp.transpose(input_matrix, (0, 1, 3, 2)).reshape(2, width, states),
        output_matrix.reshape(2, width, states),
        skip_gain.reshape(1, width),
        value_weight,
        gate_weight,
        norm_gain.reshape(1, features),
        up_weight,
        down_weight,
        jnp.asarray(perm, bf16),
        jnp.asarray(perm.T, bf16),
    )


def solution(mesh):
    in_specs = (
        P("sp", "tp"),
        P("sp", "tp"),
        P("sp", "tp"),
        P("tp", None),
        P("tp", None),
        P(None, "tp", None, None),
        P(None, "tp", None, None),
        P("tp"),
        P(None, "tp"),
        P(None, "tp"),
        P(),
        P("sp", "tp"),
        P("sp", "tp"),
    )
    body = functools.partial(per_device, mesh.shape["sp"], mesh.shape["tp"])
    return jax.shard_map(
        body, mesh=mesh, in_specs=in_specs, out_specs=P("sp", "tp"), check_vma=False
    )
```

```python
import functools

import jax
import jax.numpy as jnp
import numpy as np
from jax import lax
from jax.experimental import pallas as pl
from jax.experimental.pallas import tpu as pltpu
from jax.sharding import PartitionSpec as P

rms_eps = 1e-06
segments = 8
MESH = pl.DeviceIdType.MESH
f32, bf16 = jnp.float32, jnp.bfloat16


def sine_cosine(x):
    y = x * x
    s = 1.0 + y * (-1 / 6 + y * (1 / 120 + y * (-1 / 5040 + y * (1 / 362880 + y * (-1 / 39916800)))))
    c = 1.0 + y * (
        -0.5
        + y * (1 / 24 + y * (-1 / 720 + y * (1 / 40320 + y * (-1 / 3628800 + y * (1 / 479001600)))))
    )
    return x * s, c


def expm1_small(y):
    return y * (
        1.0
        + y * (1 / 2 + y * (1 / 6 + y * (1 / 24 + y * (1 / 120 + y * (1 / 720 + y * (1 / 5040))))))
    )


def kernel(
    n,
    ntp,
    resid_ref,
    mixer_ref,
    step_ref,
    decay_ref,
    angle_ref,
    w_in_ref,
    w_out_ref,
    skip_ref,
    value_hbm,
    gate_hbm,
    gain_ref,
    up_hbm,
    down_hbm,
    perm_ref,
    unperm_ref,
    out_ref,
    up_whole,
    down_whole,
    value_ref,
    gate_ref,
    dre,
    dim,
    fre,
    fim,
    step_wide,
    proj,
    ends,
    carries,
    mate,
    prefix,
    entry,
    mixer_perm,
    chan,
    upd,
    normed,
    hidden,
    keep,
    out1,
    in1,
    out2,
    in2,
    out3,
    in3,
    own_sem,
    z_send,
    z_recv,
    y_send,
    y_recv,
    carry_send,
    carry_recv,
    chan_core_send,
    chan_core_recv,
    chan_x_send,
    chan_x_recv,
    upd_z_send,
    upd_z_recv,
    upd_core_send,
    upd_core_recv,
    upd_x_send,
    upd_x_recv,
    sum1_send,
    sum1_recv,
    sum2_send,
    sum2_recv,
    sum3_send,
    sum3_recv,
):
    sp = lax.axis_index("sp")
    tp = lax.axis_index("tp")
    tokens, width = mixer_ref.shape
    block = up_hbm.shape[0]
    units = up_whole.shape[1]
    groups, states = decay_ref.shape
    each = width // groups
    bunch = min(128 // each, groups)
    chunks = groups // bunch
    lanes, kin = bunch * states, bunch * each
    length = tokens // segments
    pieces = z_recv.shape[2]
    piece = block // pieces
    nz, nx, per = n // 2, ntp // 2, n // ntp
    z, y = sp // 2, sp % 2
    x, core = tp // 2, tp % 2
    partner = tp + 1 - 2 * core

    def xor(a, k):
        total = 0
        bit = 1
        while bit < nz:
            digit = (a // bit) % 2
            total = total + bit * (1 - digit if k & bit else digit)
            bit *= 2
        return total

    def flip(a):
        return a + 1 - 2 * (a % 2)

    pair_z = flip(z)
    pair = 2 * pair_z + y
    inner = ((z + 1) // 2) % 2

    barrier = pltpu.get_barrier_semaphore()
    for i in range(1, n):
        pl.semaphore_signal(barrier, inc=1, device_id=((sp + i) % n, tp), device_id_type=MESH)
    for i in range(1, ntp):
        pl.semaphore_signal(barrier, inc=1, device_id=(sp, (tp + i) % ntp), device_id_type=MESH)
    pl.semaphore_wait(barrier, n - 1 + ntp - 1)

    sources, wholes = (up_hbm, down_hbm), (up_whole, down_whole)

    def rows_of(owner, part=None):
        if part is None:
            return pl.ds(pl.multiple_of(owner * block, block), block)
        return pl.ds(pl.multiple_of(owner * block + part * piece, piece), piece)

    def columns_for(a):
        return pl.ds(pl.multiple_of((a % 2) * units, units), units)

    def z_copy(which, k, zk, part, sending):
        owner = sp if sending else 2 * zk + y
        return pltpu.make_async_remote_copy(
            src_ref=sources[which].at[pl.ds(part * piece, piece), columns_for(zk)],
            dst_ref=wholes[which].at[rows_of(owner, part)],
            send_sem=z_send.at[which, k],
            recv_sem=z_recv.at[which, k, part],
            device_id=(2 * zk + y, tp),
            device_id_type=MESH,
        )

    def y_copy(which, k, zk, part, sending):
        owner = 2 * zk + (y if sending else 1 - y)
        slot = wholes[which].at[rows_of(owner, part)]
        src = slot
        if isinstance(k, int) and k == 0:
            src = sources[which].at[pl.ds(part * piece, piece), columns_for(z)]
        return pltpu.make_async_remote_copy(
            src_ref=src,
            dst_ref=slot,
            send_sem=y_send.at[which, k],
            recv_sem=y_recv.at[which, k, part],
            device_id=(2 * z + 1 - y, tp),
            device_id_type=MESH,
        )

    def z_start(which, ks, first=0, last=None):
        for part, k in [(p, k) for p in range(pieces) for k in ks][first:last]:
            z_copy(which, k, xor(z, k), part, True).start()

    beyond = range(2, nz)
    many = pieces * len(beyond)
    early, before, quarter = (5 * many) // 8, (6 * many) // 8, many // 4

    def forward(which, k, zk, first=0, last=pieces):
        for part in range(first, last):
            z_copy(which, k, zk, part, False).wait_recv()
            y_copy(which, k, zk, part, True).start()

    def y_arrived(which, k, zk):
        for part in range(pieces):
            y_copy(which, k, zk, part, False).wait_recv()

    far = []
    for base in range(2, nz, 2):
        zb = xor(z, base)
        zf = flip(zb)
        far.append((base + inner, zb + inner * (zf - zb)))
        far.append((base + 1 - inner, zf + inner * (zb - zf)))
    near, distant = far[0::2], far[1::2]

    own = []
    for which in range(2):
        c = pltpu.make_async_copy(
            sources[which].at[:, columns_for(z)], wholes[which].at[rows_of(sp)], own_sem.at[which]
        )
        c.start()
        own.append(c)
    for part in range(pieces):
        y_copy(0, 0, z, part, True).start()
    z_start(0, (1,))
    ahead = pieces // 2

    @pl.when(inner == 0)
    def _():
        z_start(1, (1,), 0, ahead)

    @pl.when(inner == 1)
    def _():
        z_start(0, beyond, 0, early)

    gates = []
    for which, (source, target) in enumerate(((value_hbm, value_ref), (gate_hbm, gate_ref))):
        c = pltpu.make_async_copy(source, target, own_sem.at[2 + which])
        c.start()
        gates.append(c)

    def tp_at(a, b):
        return 2 * a + b

    def chan_core(i, c, sending):
        cols = pl.ds(c * kin, kin)
        slot = tp_at((x + nx - i) % nx, core if sending else 1 - core)
        return pltpu.make_async_remote_copy(
            src_ref=chan.at[slot, :, cols],
            dst_ref=chan.at[slot, :, cols],
            send_sem=chan_core_send.at[i, c],
            recv_sem=chan_core_recv.at[i, c],
            device_id=(sp, partner),
            device_id_type=MESH,
        )

    def chan_x(i, c, sending):
        cols = pl.ds(c * kin, kin)
        slot = tp if sending else tp_at((x + nx - i) % nx, core)
        return pltpu.make_async_remote_copy(
            src_ref=chan.at[slot, :, cols],
            dst_ref=chan.at[slot, :, cols],
            send_sem=chan_x_send.at[i - 1, c],
            recv_sem=chan_x_recv.at[i - 1, c],
            device_id=(sp, tp_at((x + i) % nx, core)),
            device_id_type=MESH,
        )

    def chan_forward(c):
        for i in range(1, nx):
            chan_x(i, c, False).wait_recv()
            chan_core(i, c, True).start()

    mixer_perm[...] = jnp.dot(
        perm_ref[...], mixer_ref[...], preferred_element_type=f32
    ).astype(bf16)
    highest = lax.Precision.HIGHEST
    step_size = lax.dot_general(
        perm_ref[...].astype(f32),
        jnp.exp(step_ref[...]),
        (((1,), (1,)), ((), ())),
        precision=highest,
        preferred_element_type=f32,
    )

    def iota(shape, axis):
        return lax.broadcasted_iota(jnp.int32, shape, axis)

    def ones_where(mask, dtype=f32):
        return jnp.where(mask, 1.0, 0.0).astype(dtype)

    def belongs(rows, columns, span, first):
        gap = iota((rows, columns), 1) + first - iota((rows, columns), 0) * span
        return ones_where((gap >= 0) & (gap < span))

    def tiled(size, copies):
        shape = (size, size * copies)
        hits = jnp.zeros(shape, f32)
        for i in range(copies):
            hits += ones_where(iota(shape, 1) - iota(shape, 0) == i * size)
        return hits

    over_states = tiled(states, bunch)
    agree = jnp.zeros((kin, lanes), f32)
    for i in range(bunch):
        r, l = iota((kin, lanes), 0) - i * each, iota((kin, lanes), 1) - i * states
        agree += ones_where((r >= 0) & (r < each) & (l >= 0) & (l < states))

    def wide_rate(table, c):
        spread = jnp.dot(table, over_states, precision=highest, preferred_element_type=f32)
        return jnp.sum(
            spread * belongs(groups, lanes, states, c * lanes), axis=0, keepdims=True
        )

    for c in range(chunks):
        cols = pl.ds(c * lanes, lanes)
        step_wide[...] = jnp.dot(
            step_size,
            belongs(groups, lanes, states, c * lanes),
            precision=highest,
            preferred_element_type=f32,
        )
        for i in range(2):
            matrix = jnp.dot(
                w_in_ref[i, c * kin : (c + 1) * kin, :].astype(bf16),
                over_states.astype(bf16),
                preferred_element_type=f32,
            )
            proj[:, i * lanes : (i + 1) * lanes] = jnp.dot(
                mixer_perm[:, c * kin : (c + 1) * kin],
                (matrix * agree).astype(bf16),
                preferred_element_type=f32,
            )
        rate_row = wide_rate(decay_ref[...], c)
        angle_row = wide_rate(angle_ref[...], c)
        modulus = rate_row * rate_row + angle_row * angle_row
        shape = (segments, lanes)
        rate = jnp.broadcast_to(rate_row, shape)
        half_angle = jnp.broadcast_to(angle_row * 0.5, shape)
        rate_n = jnp.broadcast_to(rate_row / modulus, shape)
        angle_n = jnp.broadcast_to(angle_row / modulus, shape)

        def one(j, state):
            pr, pi, sr, si = state
            rows = pl.ds(pl.multiple_of(j * segments, segments), segments)
            step = step_wide[rows, :]
            s, co = sine_cosine(half_angle * step)
            em = expm1_small(-rate * step)
            factor = 1.0 + em
            twice = 2.0 * s * s
            cos_r = 1.0 - twice
            dr = factor * cos_r
            di = factor * (2.0 * s * co)
            mr = em * cos_r - twice
            vr = di * angle_n - mr * rate_n
            vi = -di * rate_n - mr * angle_n
            a = proj[rows, 0:lanes]
            b = proj[rows, lanes : 2 * lanes]
            fr = vr * a - vi * b
            fi = vr * b + vi * a
            dre[rows, cols] = dr
            dim[rows, cols] = di
            fre[rows, cols] = fr
            fim[rows, cols] = fi
            return (
                dr * pr - di * pi,
                dr * pi + di * pr,
                dr * sr - di * si + fr,
                dr * si + di * sr + fi,
            )

        zero = jnp.zeros(shape, f32)
        last = lax.fori_loop(0, length, one, (zero + 1.0, zero, zero, zero), unroll=2)
        for i in range(4):
            ends[i, :, cols] = last[i]

    def link(earlier, later):
        return (
            later[0] * earlier[0] - later[1] * earlier[1] + later[2],
            later[0] * earlier[1] + later[1] * earlier[0] + later[3],
        )

    def chain(first, second):
        fr, fi, ur, ui = first
        qr, qi, tr, ti = second
        vr, vi = link((ur, ui), second)
        return qr * fr - qi * fi, qr * fi + qi * fr, vr, vi

    def four(ref, *at):
        return tuple(ref[(*at, slice(i, i + 1), slice(None))] for i in range(4))

    whole_run = tuple(ends[i, 0:1, :] for i in range(4))
    for s in range(1, segments):
        whole_run = chain(whole_run, tuple(ends[i, s : s + 1, :] for i in range(4)))
    for i, v in enumerate(whole_run):
        mate[y, i : i + 1, :] = v

    def mate_copy(sending):
        slot = y if sending else 1 - y
        return pltpu.make_async_remote_copy(
            src_ref=mate.at[slot],
            dst_ref=mate.at[slot],
            send_sem=carry_send.at[0],
            recv_sem=carry_recv.at[0],
            device_id=(2 * z + 1 - y, tp),
            device_id_type=MESH,
        )

    def carry_copy(i, sending):
        slot = z if sending else (z + nz - i) % nz
        return pltpu.make_async_remote_copy(
            src_ref=carries.at[slot],
            dst_ref=carries.at[slot],
            send_sem=carry_send.at[i],
            recv_sem=carry_recv.at[i],
            device_id=(2 * ((z + i) % nz) + y, tp),
            device_id_type=MESH,
        )

    upper = z // (nz // 2)

    def second_sends():
        @pl.when(inner == 1)
        def _():
            z_start(0, beyond, early)

        @pl.when(inner == 0)
        def _():
            z_start(0, beyond, 0, before)

    pl.when(upper == 1)(second_sends)
    mate_copy(True).start()
    for part in range(pieces):
        y_copy(1, 0, z, part, True).start()
    mate_copy(False).wait_recv()
    for i, v in enumerate(chain(four(mate, 0), four(mate, 1))):
        carries[z, i : i + 1, :] = v
    for i in range(1, nz):

        @pl.when(z + i < nz)
        def _():
            carry_copy(i, True).start()

    prefix[...] = jnp.zeros_like(prefix)

    def extend(run):
        for i, v in enumerate(link((prefix[0:1, :], prefix[1:2, :]), run)):
            prefix[i : i + 1, :] = v

    for i in range(1, nz):

        @pl.when(z >= i)
        def _():
            carry_copy(i, False).wait_recv()

    for i in range(1, nz):

        @pl.when(z + i < nz)
        def _():
            carry_copy(i, True).wait_send()

    pl.when(upper == 0)(second_sends)

    for d in range(nz - 1):

        @pl.when(d < z)
        def _():
            extend(four(carries, d))

    @pl.when(y == 1)
    def _():
        extend(four(mate, 0))

    cr, ci = prefix[0:1, :], prefix[1:2, :]
    for s in range(segments):
        entry[0, s : s + 1, :] = cr
        entry[1, s : s + 1, :] = ci
        cr, ci = link((cr, ci), tuple(ends[i, s : s + 1, :] for i in range(4)))
    forward(0, 1, pair_z)
    half_way = pieces // 2
    for k, zk in near:
        forward(0, k, zk, 0, half_way)

    for c in range(chunks):
        cols = pl.ds(c * lanes, lanes)

        def again(j, state):
            rows = pl.ds(pl.multiple_of(j * segments, segments), segments)
            dr, di = dre[rows, cols], dim[rows, cols]
            xr, xi = link(state, (dr, di, fre[rows, cols], fim[rows, cols]))
            proj[rows, 0:lanes] = xr
            proj[rows, lanes : 2 * lanes] = xi
            return xr, xi

        lax.fori_loop(0, length, again, (entry[0, :, cols], entry[1, :, cols]), unroll=4)
        ins = slice(c * kin, (c + 1) * kin)
        mech = jnp.zeros((tokens, kin), f32)
        for i in range(2):
            matrix = jnp.dot(
                w_out_ref[i, c * kin : (c + 1) * kin, :].astype(bf16),
                over_states.astype(bf16),
                preferred_element_type=f32,
            )
            mech += (1 - 2 * i) * lax.dot_general(
                proj[:, i * lanes : (i + 1) * lanes].astype(bf16),
                (matrix * agree).astype(bf16),
                (((1,), (1,)), ((), ())),
                preferred_element_type=f32,
            )
        mech = mech + skip_ref[0:1, ins] * mixer_perm[:, ins].astype(f32)
        mixed = jax.nn.gelu(mech).astype(bf16)
        chan[tp, :, ins] = jnp.dot(
            unperm_ref[...], mixed, preferred_element_type=f32
        ).astype(bf16)
        chan_core(0, c, True).start()
        for i in range(1, nx):
            chan_x(i, c, True).start()
        if c >= 2:
            chan_forward(c - 2)

    for c in range(max(chunks - 2, 0), chunks):
        chan_forward(c)
    for c in gates:
        c.wait()
    for c in range(chunks):
        for i in range(nx):
            chan_core(i, c, False).wait_recv()

    tile = 256

    @pl.loop(0, width // tile)
    def _(t):
        cols = pl.ds(pl.multiple_of(t * tile, tile), tile)
        v = jnp.zeros((tokens, tile), f32)
        g = jnp.zeros((tokens, tile), f32)
        for q in range(ntp):
            rows = slice(q * width, (q + 1) * width)
            v += jnp.dot(chan[q], value_ref[rows, cols], preferred_element_type=f32)
            g += jnp.dot(chan[q], gate_ref[rows, cols], preferred_element_type=f32)
        upd[0, tp, :, cols] = (resid_ref[:, cols].astype(f32) + v * jax.nn.sigmoid(g)).astype(bf16)

    def upd_z():
        return pltpu.make_async_remote_copy(
            src_ref=upd.at[0, tp],
            dst_ref=upd.at[1, tp],
            send_sem=upd_z_send.at[0],
            recv_sem=upd_z_recv.at[0],
            device_id=(pair, tp),
            device_id_type=MESH,
        )

    def upd_x(i, h, sending):
        slot = tp if sending else tp_at((x + nx - i) % nx, core)
        return pltpu.make_async_remote_copy(
            src_ref=upd.at[h, slot],
            dst_ref=upd.at[h, slot],
            send_sem=upd_x_send.at[i - 1, h],
            recv_sem=upd_x_recv.at[i - 1, h],
            device_id=(sp, tp_at((x + i) % nx, core)),
            device_id_type=MESH,
        )

    def upd_core(i, h, sending):
        slot = tp_at((x + nx - i) % nx, core if sending else 1 - core)
        return pltpu.make_async_remote_copy(
            src_ref=upd.at[h, slot],
            dst_ref=upd.at[h, slot],
            send_sem=upd_core_send.at[i, h],
            recv_sem=upd_core_recv.at[i, h],
            device_id=(sp, partner),
            device_id_type=MESH,
        )

    upd_z().start()
    for i in range(1, nx):
        upd_x(i, 0, True).start()
    upd_core(0, 0, True).start()

    @pl.when(inner == 0)
    def _():
        z_start(0, beyond, before)
        for k in beyond:
            z_start(1, (k,))
        z_start(1, (1,), ahead)

    @pl.when(inner == 1)
    def _():
        z_start(1, beyond, 0, quarter)
        z_start(1, (1,), 0)

    most = (3 * pieces) // 4
    for k, zk in distant:
        forward(0, k, zk, 0, most)
    for k, zk in near:
        forward(0, k, zk, half_way)
    for i in range(1, nx):
        upd_x(i, 0, False).wait_recv()
        upd_core(i, 0, True).start()
    upd_z().wait_recv()
    for i in range(1, nx):
        upd_x(i, 1, True).start()
    upd_core(0, 1, True).start()
    for k, zk in distant:
        forward(0, k, zk, most)

    def normalize(h):
        for i in range(nx):
            upd_core(i, h, False).wait_recv()
        total = jnp.zeros((tokens, 1), f32)
        for q in range(ntp):
            u = upd[h, q].astype(f32)
            total += jnp.sum(u * u, axis=1, keepdims=True)
        inv = lax.rsqrt(total * (1.0 / (width * ntp)) + rms_eps)
        for q in range(ntp):
            cols = slice(q * width, (q + 1) * width)
            normed[h * tokens : (h + 1) * tokens, cols] = (upd[h, q].astype(f32) * inv * gain_ref[0:1, cols]).astype(bf16)

    normalize(0)
    for i in range(1, nx):
        upd_x(i, 1, False).wait_recv()
        upd_core(i, 1, True).start()
    normalize(1)

    @pl.when(inner == 1)
    def _():
        forward(1, 1, pair_z, 0, ahead)

    @pl.when(inner == 0)
    def _():
        forward(1, 1, pair_z)

    for c in own:
        c.wait()
    y_arrived(0, 0, z)
    y_arrived(0, 1, pair_z)
    for k, zk in far:
        y_arrived(0, k, zk)

    @pl.loop(0, units // tile)
    def _(t):
        cols = pl.ds(pl.multiple_of(t * tile, tile), tile)
        for h in range(2):
            some = slice(h * tokens, (h + 1) * tokens)
            r = jnp.dot(normed[some, :], up_whole[:, cols], preferred_element_type=f32)
            r = jnp.maximum(r, 0.0)
            hidden[some, cols] = (r * r).astype(bf16)

    cuts = sum1_send.shape[1]
    cut = block // cuts

    def strip(h):
        return slice(h * cut, (h + 1) * cut)

    def sum1(s, h):
        return pltpu.make_async_remote_copy(
            src_ref=out1.at[s, :, pl.ds(h * cut, cut)],
            dst_ref=in1.at[s, :, pl.ds(h * cut, cut)],
            send_sem=sum1_send.at[s, h],
            recv_sem=sum1_recv.at[s, h],
            device_id=(sp, partner),
            device_id_type=MESH,
        )

    def sum2(s, h):
        return pltpu.make_async_remote_copy(
            src_ref=out2.at[s, :, pl.ds(h * cut, cut)],
            dst_ref=in2.at[s, :, pl.ds(h * cut, cut)],
            send_sem=sum2_send.at[s, h],
            recv_sem=sum2_recv.at[s, h],
            device_id=(pair, tp),
            device_id_type=MESH,
        )

    def sum3(s, h, there, to):
        return pltpu.make_async_remote_copy(
            src_ref=out3.at[s, :, pl.ds(h * cut, cut)],
            dst_ref=in3.at[s % per, there, :, pl.ds(h * cut, cut)],
            send_sem=sum3_send.at[s, h],
            recv_sem=sum3_recv.at[s % per, there, h],
            device_id=(sp, to),
            device_id_type=MESH,
        )

    def core_of(s):
        return (s // per) % 2

    def x_of(s):
        return s // per // 2

    def stage1(s, first=0, last=cuts):
        rows = pl.ds(pl.multiple_of(s * block + first * cut, cut), (last - first) * cut)

        @pl.loop(0, 2)
        def _(half):
            some = pl.ds(pl.multiple_of(half * tokens, tokens), tokens)
            keep[s, some, first * cut : last * cut] = lax.dot_general(
                hidden[some, :],
                down_whole[rows, :],
                (((1,), (1,)), ((), ())),
                preferred_element_type=f32,
            )

        @pl.when(core_of(s) != core)
        def _():
            for h in range(first, last):
                out1[s, :, strip(h)] = keep[s, :, strip(h)].astype(bf16)
                sum1(s, h).start()

    def stage2(s, first=0, last=cuts):
        @pl.when(core_of(s) == core)
        def _():
            for h in range(first, last):
                w = strip(h)
                sum1(s, h).wait_recv()
                out2[s, :, w] = (keep[s, tokens:, w] + in1[s, tokens:, w].astype(f32)).astype(bf16)
                sum2(s, h).start()
                keep[s, :tokens, w] = keep[s, :tokens, w] + in1[s, :tokens, w].astype(f32)

    def stage3(s, first=0, last=cuts):
        @pl.when(core_of(s) == core)
        def _():
            for h in range(first, last):
                w = strip(h)
                sum2(s, h).wait_recv()
                total = keep[s, :tokens, w] + in2[s, :, w].astype(f32)

                @pl.when(x_of(s) == x)
                def _():
                    keep[s, :tokens, w] = total

                @pl.when(x_of(s) != x)
                def _():
                    out3[s, :, w] = total.astype(bf16)
                    sum3(s, h, x, s // per).start()

    def step(k, zk, side, eager=False):
        if side == 1:
            y_arrived(1, k, zk)
        s = 2 * zk + (y if side == 0 else 1 - y)
        stage1(s)
        if waiting:
            stage2(waiting.pop())
        if eager:
            stage2(s)
        else:
            waiting.append(s)
        order.append(s)

    order, waiting = [], []

    def weights_sent(which):
        slot = wholes[which].at[rows_of(sp)]
        for k in range(nz):
            for sem in (y_send, z_send)[: 1 + (k > 0)]:
                pltpu.make_async_remote_copy(
                    src_ref=slot,
                    dst_ref=slot,
                    send_sem=sem.at[which, k],
                    recv_sem=z_recv.at[which, k, 0],
                    device_id=(2 * z + 1 - y, tp),
                    device_id_type=MESH,
                ).wait_send()

    def first_sent():
        weights_sent(0)
        mate_copy(True).wait_send()
        for i in range(nx):
            for c in range(chunks):
                chan_core(i, c, True).wait_send()
                if i > 0:
                    chan_x(i, c, True).wait_send()
            for h in range(2):
                upd_core(i, h, True).wait_send()
                if i > 0:
                    upd_x(i, h, True).wait_send()
        upd_z().wait_send()

    for k, zk in distant:
        forward(1, k, zk, 0, half_way)
    for side in range(2):
        step(0, z, side)

    @pl.when(inner == 1)
    def _():
        z_start(1, beyond, quarter)

    for k, zk in distant:
        forward(1, k, zk, half_way)

    for k, zk in near:
        forward(1, k, zk, 0, pieces // 4)
    for k, zk in distant:
        for side in range(2):
            step(k, zk, side)
    stage2(waiting.pop())

    @pl.when(inner == 1)
    def _():
        forward(1, 1, pair_z, ahead)

    for k, zk in near:
        forward(1, k, zk, pieces // 4, half_way)
    step(1, pair_z, 0, True)
    for k, zk in near:
        forward(1, k, zk, half_way, most)
    for s in order[2:-1]:
        stage3(s)
    step(1, pair_z, 1, True)
    first_sent()
    for k, zk in near:
        forward(1, k, zk, most)
    remaining = order[:2] + order[-2:]
    ending = []
    for k, zk in near:
        step(k, zk, 0, True)
        ending.append(2 * zk + y)
    for s in remaining:
        stage3(s)
    for h in range(cuts):
        for k, zk in near:
            for part in range(h * pieces // cuts, (h + 1) * pieces // cuts):
                y_copy(1, k, zk, part, False).wait_recv()
            s = 2 * zk + 1 - y
            stage1(s, h, h + 1)
            stage2(s, h, h + 1)
        if h == 0:
            for e in ending:
                stage3(e)
    weights_sent(1)
    for s in range(n):

        @pl.when(core_of(s) != core)
        def _():
            for h in range(cuts):
                sum1(s, h).wait_send()

    for h in range(cuts):
        for _, zk in near:
            stage3(2 * zk + 1 - y, h, h + 1)
    for s in range(n):

        @pl.when(core_of(s) == core)
        def _():
            for h in range(cuts):
                sum2(s, h).wait_send()

    for j in range(per):
        s = tp * per + j
        cols = slice(j * block, (j + 1) * block)
        total = keep[s, :tokens]
        for i in range(1, nx):
            there = (x + i) % nx
            for h in range(cuts):
                sum3(s, h, there, tp_at(there, core)).wait_recv()
            total += in3[j, there].astype(f32)
        out_ref[:, cols] = (upd[0, tp, :, cols].astype(f32) + total).astype(bf16)

    for s in range(n):

        @pl.when((core_of(s) == core) & (x_of(s) != x))
        def _():
            for h in range(cuts):
                sum3(s, h, x, s // per).wait_send()


def per_device(
    n,
    ntp,
    resid,
    mixer_in,
    log_step,
    decay_real,
    frequency,
    input_matrix,
    output_matrix,
    skip_gain,
    value_weight,
    gate_weight,
    norm_gain,
    up_weight,
    down_weight,
):
    tokens, width = mixer_in.shape
    groups, states = decay_real.shape
    each = width // groups
    bunch = min(128 // each, groups)
    chunks = groups // bunch
    lanes = bunch * states
    features, units = value_weight.shape[0], up_weight.shape[1] // 2
    block = up_weight.shape[0]
    length = tokens // segments
    row = np.arange(tokens)
    perm = (row[None, :] == ((row % segments) * length + row // segments)[:, None]).astype(np.float32)
    nz, nx, per, pieces = n // 2, ntp // 2, n // ntp, 4
    total = groups * states
    cuts = 2 if block % 256 == 0 else 1
    dma = pltpu.SemaphoreType.DMA
    vmem = pl.BlockSpec(memory_space=pltpu.VMEM)
    hbm = pl.BlockSpec(memory_space=pl.ANY)
    return pl.pallas_call(
        functools.partial(kernel, n, ntp),
        out_shape=jax.ShapeDtypeStruct((tokens, width), bf16),
        in_specs=[vmem] * 8 + [hbm] * 2 + [vmem] + [hbm] * 2 + [vmem] * 2,
        out_specs=vmem,
        scratch_shapes=[
            pltpu.VMEM((features, units), bf16),
            pltpu.VMEM((features, units), bf16),
            pltpu.VMEM((features, width), bf16),
            pltpu.VMEM((features, width), bf16),
            pltpu.VMEM((tokens, total), f32),
            pltpu.VMEM((tokens, total), f32),
            pltpu.VMEM((tokens, total), f32),
            pltpu.VMEM((tokens, total), f32),
            pltpu.VMEM((tokens, lanes), f32),
            pltpu.VMEM((tokens, 2 * lanes), f32),
            pltpu.VMEM((4, segments, total), f32),
            pltpu.VMEM((nz, 4, total), f32),
            pltpu.VMEM((2, 4, total), f32),
            pltpu.VMEM((2, total), f32),
            pltpu.VMEM((2, segments, total), f32),
            pltpu.VMEM((tokens, width), bf16),
            pltpu.VMEM((ntp, tokens, width), bf16),
            pltpu.VMEM((2, ntp, tokens, width), bf16),
            pltpu.VMEM((2 * tokens, features), bf16),
            pltpu.VMEM((2 * tokens, units), bf16),
            pltpu.VMEM((n, 2 * tokens, block), f32),
            pltpu.VMEM((n, 2 * tokens, block), bf16),
            pltpu.VMEM((n, 2 * tokens, block), bf16),
            pltpu.VMEM((n, tokens, block), bf16),
            pltpu.VMEM((n, tokens, block), bf16),
            pltpu.VMEM((n, tokens, block), bf16),
            pltpu.VMEM((per, nx, tokens, block), bf16),
            dma((4,)),
            dma((2, nz)),
            dma((2, nz, pieces)),
            dma((2, nz)),
            dma((2, nz, pieces)),
            dma((nz,)),
            dma((nz,)),
            dma((nx, chunks)),
            dma((nx, chunks)),
            dma((max(nx - 1, 1), chunks)),
            dma((max(nx - 1, 1), chunks)),
            dma((1,)),
            dma((1,)),
            dma((nx, 2)),
            dma((nx, 2)),
            dma((max(nx - 1, 1), 2)),
            dma((max(nx - 1, 1), 2)),
            dma((n, cuts)),
            dma((n, cuts)),
            dma((n, cuts)),
            dma((n, cuts)),
            dma((n, cuts)),
            dma((per, nx, cuts)),
        ],
        compiler_params=pltpu.CompilerParams(
            collective_id=0, has_side_effects=True, vmem_limit_bytes=64 * 1024 * 1024 - 65536
        ),
    )(
        resid,
        mixer_in,
        log_step.T,
        decay_real,
        frequency,
        jnp.transpose(input_matrix, (0, 1, 3, 2)).reshape(2, width, states),
        output_matrix.reshape(2, width, states),
        skip_gain.reshape(1, width),
        value_weight,
        gate_weight,
        norm_gain.reshape(1, features),
        up_weight,
        down_weight,
        jnp.asarray(perm, bf16),
        jnp.asarray(perm.T, bf16),
    )


def solution(mesh):
    in_specs = (
        P("sp", "tp"),
        P("sp", "tp"),
        P("sp", "tp"),
        P("tp", None),
        P("tp", None),
        P(None, "tp", None, None),
        P(None, "tp", None, None),
        P("tp"),
        P(None, "tp"),
        P(None, "tp"),
        P(),
        P("sp", "tp"),
        P("sp", "tp"),
    )
    body = functools.partial(per_device, mesh.shape["sp"], mesh.shape["tp"])
    return jax.shard_map(
        body, mesh=mesh, in_specs=in_specs, out_specs=P("sp", "tp"), check_vma=False
    )
```

```python
import functools

import jax
import jax.numpy as jnp
import numpy as np
from jax import lax
from jax.experimental import pallas as pl
from jax.experimental.pallas import tpu as pltpu
from jax.sharding import PartitionSpec as P

rms_eps = 1e-06
segments = 8
MESH = pl.DeviceIdType.MESH
f32, bf16 = jnp.float32, jnp.bfloat16


def sine_cosine(x):
    y = x * x
    s = 1.0 + y * (-1 / 6 + y * (1 / 120 + y * (-1 / 5040 + y * (1 / 362880 + y * (-1 / 39916800)))))
    c = 1.0 + y * (
        -0.5
        + y * (1 / 24 + y * (-1 / 720 + y * (1 / 40320 + y * (-1 / 3628800 + y * (1 / 479001600)))))
    )
    return x * s, c


def expm1_small(y):
    return y * (
        1.0
        + y * (1 / 2 + y * (1 / 6 + y * (1 / 24 + y * (1 / 120 + y * (1 / 720 + y * (1 / 5040))))))
    )


def kernel(
    n,
    ntp,
    resid_ref,
    mixer_ref,
    step_ref,
    decay_ref,
    angle_ref,
    w_in_ref,
    w_out_ref,
    skip_ref,
    value_hbm,
    gate_hbm,
    gain_ref,
    up_hbm,
    down_hbm,
    perm_ref,
    unperm_ref,
    out_ref,
    up_whole,
    down_whole,
    value_ref,
    gate_ref,
    dre,
    dim,
    fre,
    fim,
    step_wide,
    proj,
    ends,
    carries,
    mate,
    prefix,
    entry,
    mixer_perm,
    chan,
    upd,
    normed,
    hidden,
    keep,
    out1,
    in1,
    out2,
    in2,
    out3,
    in3,
    own_sem,
    z_send,
    z_recv,
    y_send,
    y_recv,
    carry_send,
    carry_recv,
    chan_core_send,
    chan_core_recv,
    chan_x_send,
    chan_x_recv,
    upd_z_send,
    upd_z_recv,
    upd_core_send,
    upd_core_recv,
    upd_x_send,
    upd_x_recv,
    sum1_send,
    sum1_recv,
    sum2_send,
    sum2_recv,
    sum3_send,
    sum3_recv,
):
    sp = lax.axis_index("sp")
    tp = lax.axis_index("tp")
    tokens, width = mixer_ref.shape
    block = up_hbm.shape[0]
    units = up_whole.shape[1]
    groups, states = decay_ref.shape
    each = width // groups
    bunch = min(128 // each, groups)
    chunks = groups // bunch
    lanes, kin = bunch * states, bunch * each
    length = tokens // segments
    pieces = z_recv.shape[2]
    piece = block // pieces
    nz, nx, per = n // 2, ntp // 2, n // ntp
    z, y = sp // 2, sp % 2
    x, core = tp // 2, tp % 2
    partner = tp + 1 - 2 * core

    def xor(a, k):
        total = 0
        bit = 1
        while bit < nz:
            digit = (a // bit) % 2
            total = total + bit * (1 - digit if k & bit else digit)
            bit *= 2
        return total

    def flip(a):
        return a + 1 - 2 * (a % 2)

    pair_z = flip(z)
    pair = 2 * pair_z + y
    inner = ((z + 1) // 2) % 2

    barrier = pltpu.get_barrier_semaphore()
    for i in range(1, n):
        pl.semaphore_signal(barrier, inc=1, device_id=((sp + i) % n, tp), device_id_type=MESH)
    for i in range(1, ntp):
        pl.semaphore_signal(barrier, inc=1, device_id=(sp, (tp + i) % ntp), device_id_type=MESH)
    pl.semaphore_wait(barrier, n - 1 + ntp - 1)

    sources, wholes = (up_hbm, down_hbm), (up_whole, down_whole)

    def rows_of(owner, part=None):
        if part is None:
            return pl.ds(pl.multiple_of(owner * block, block), block)
        return pl.ds(pl.multiple_of(owner * block + part * piece, piece), piece)

    def columns_for(a):
        return pl.ds(pl.multiple_of((a % 2) * units, units), units)

    def z_copy(which, k, zk, part, sending):
        owner = sp if sending else 2 * zk + y
        return pltpu.make_async_remote_copy(
            src_ref=sources[which].at[pl.ds(part * piece, piece), columns_for(zk)],
            dst_ref=wholes[which].at[rows_of(owner, part)],
            send_sem=z_send.at[which, k],
            recv_sem=z_recv.at[which, k, part],
            device_id=(2 * zk + y, tp),
            device_id_type=MESH,
        )

    def y_copy(which, k, zk, part, sending):
        owner = 2 * zk + (y if sending else 1 - y)
        slot = wholes[which].at[rows_of(owner, part)]
        src = slot
        if isinstance(k, int) and k == 0:
            src = sources[which].at[pl.ds(part * piece, piece), columns_for(z)]
        return pltpu.make_async_remote_copy(
            src_ref=src,
            dst_ref=slot,
            send_sem=y_send.at[which, k],
            recv_sem=y_recv.at[which, k, part],
            device_id=(2 * z + 1 - y, tp),
            device_id_type=MESH,
        )

    def z_start(which, ks, first=0, last=None):
        for part, k in [(p, k) for p in range(pieces) for k in ks][first:last]:
            z_copy(which, k, xor(z, k), part, True).start()

    beyond = range(2, nz)
    many = pieces * len(beyond)
    early, before, quarter = (5 * many) // 8, (6 * many) // 8, many // 4

    def forward(which, k, zk, first=0, last=pieces):
        for part in range(first, last):
            z_copy(which, k, zk, part, False).wait_recv()
            y_copy(which, k, zk, part, True).start()

    def y_arrived(which, k, zk):
        for part in range(pieces):
            y_copy(which, k, zk, part, False).wait_recv()

    far = []
    for base in range(2, nz, 2):
        zb = xor(z, base)
        zf = flip(zb)
        far.append((base + inner, zb + inner * (zf - zb)))
        far.append((base + 1 - inner, zf + inner * (zb - zf)))
    near, distant = far[0::2], far[1::2]

    own = []
    for which in range(2):
        c = pltpu.make_async_copy(
            sources[which].at[:, columns_for(z)], wholes[which].at[rows_of(sp)], own_sem.at[which]
        )
        c.start()
        own.append(c)
    for part in range(pieces):
        y_copy(0, 0, z, part, True).start()
    z_start(0, (1,))
    ahead = pieces // 2

    @pl.when(inner == 0)
    def _():
        z_start(1, (1,), 0, ahead)

    @pl.when(inner == 1)
    def _():
        z_start(0, beyond, 0, early)

    gates = []
    for which, (source, target) in enumerate(((value_hbm, value_ref), (gate_hbm, gate_ref))):
        c = pltpu.make_async_copy(source, target, own_sem.at[2 + which])
        c.start()
        gates.append(c)

    def tp_at(a, b):
        return 2 * a + b

    def chan_core(i, c, sending):
        cols = pl.ds(c * kin, kin)
        slot = tp_at((x + nx - i) % nx, core if sending else 1 - core)
        return pltpu.make_async_remote_copy(
            src_ref=chan.at[slot, :, cols],
            dst_ref=chan.at[slot, :, cols],
            send_sem=chan_core_send.at[i, c],
            recv_sem=chan_core_recv.at[i, c],
            device_id=(sp, partner),
            device_id_type=MESH,
        )

    def chan_x(i, c, sending):
        cols = pl.ds(c * kin, kin)
        slot = tp if sending else tp_at((x + nx - i) % nx, core)
        return pltpu.make_async_remote_copy(
            src_ref=chan.at[slot, :, cols],
            dst_ref=chan.at[slot, :, cols],
            send_sem=chan_x_send.at[i - 1, c],
            recv_sem=chan_x_recv.at[i - 1, c],
            device_id=(sp, tp_at((x + i) % nx, core)),
            device_id_type=MESH,
        )

    def chan_forward(c):
        for i in range(1, nx):
            chan_x(i, c, False).wait_recv()
            chan_core(i, c, True).start()

    mixer_perm[...] = jnp.dot(
        perm_ref[...], mixer_ref[...], preferred_element_type=f32
    ).astype(bf16)
    highest = lax.Precision.HIGHEST
    step_size = lax.dot_general(
        perm_ref[...].astype(f32),
        jnp.exp(step_ref[...]),
        (((1,), (1,)), ((), ())),
        precision=highest,
        preferred_element_type=f32,
    )

    def iota(shape, axis):
        return lax.broadcasted_iota(jnp.int32, shape, axis)

    def ones_where(mask, dtype=f32):
        return jnp.where(mask, 1.0, 0.0).astype(dtype)

    def belongs(rows, columns, span, first):
        gap = iota((rows, columns), 1) + first - iota((rows, columns), 0) * span
        return ones_where((gap >= 0) & (gap < span))

    def tiled(size, copies):
        shape = (size, size * copies)
        hits = jnp.zeros(shape, f32)
        for i in range(copies):
            hits += ones_where(iota(shape, 1) - iota(shape, 0) == i * size)
        return hits

    over_states = tiled(states, bunch)
    agree = jnp.zeros((kin, lanes), f32)
    for i in range(bunch):
        r, l = iota((kin, lanes), 0) - i * each, iota((kin, lanes), 1) - i * states
        agree += ones_where((r >= 0) & (r < each) & (l >= 0) & (l < states))

    def wide_rate(table, c):
        spread = jnp.dot(table, over_states, precision=highest, preferred_element_type=f32)
        return jnp.sum(
            spread * belongs(groups, lanes, states, c * lanes), axis=0, keepdims=True
        )

    for c in range(chunks):
        cols = pl.ds(c * lanes, lanes)
        step_wide[...] = jnp.dot(
            step_size,
            belongs(groups, lanes, states, c * lanes),
            precision=highest,
            preferred_element_type=f32,
        )
        for i in range(2):
            matrix = jnp.dot(
                w_in_ref[i, c * kin : (c + 1) * kin, :].astype(bf16),
                over_states.astype(bf16),
                preferred_element_type=f32,
            )
            proj[:, i * lanes : (i + 1) * lanes] = jnp.dot(
                mixer_perm[:, c * kin : (c + 1) * kin],
                (matrix * agree).astype(bf16),
                preferred_element_type=f32,
            )
        rate_row = wide_rate(decay_ref[...], c)
        angle_row = wide_rate(angle_ref[...], c)
        modulus = rate_row * rate_row + angle_row * angle_row
        shape = (segments, lanes)
        rate = jnp.broadcast_to(rate_row, shape)
        half_angle = jnp.broadcast_to(angle_row * 0.5, shape)
        rate_n = jnp.broadcast_to(rate_row / modulus, shape)
        angle_n = jnp.broadcast_to(angle_row / modulus, shape)

        def one(j, state):
            pr, pi, sr, si = state
            rows = pl.ds(pl.multiple_of(j * segments, segments), segments)
            step = step_wide[rows, :]
            s, co = sine_cosine(half_angle * step)
            em = expm1_small(-rate * step)
            factor = 1.0 + em
            twice = 2.0 * s * s
            cos_r = 1.0 - twice
            dr = factor * cos_r
            di = factor * (2.0 * s * co)
            mr = em * cos_r - twice
            vr = di * angle_n - mr * rate_n
            vi = -di * rate_n - mr * angle_n
            a = proj[rows, 0:lanes]
            b = proj[rows, lanes : 2 * lanes]
            fr = vr * a - vi * b
            fi = vr * b + vi * a
            dre[rows, cols] = dr
            dim[rows, cols] = di
            fre[rows, cols] = fr
            fim[rows, cols] = fi
            return (
                dr * pr - di * pi,
                dr * pi + di * pr,
                dr * sr - di * si + fr,
                dr * si + di * sr + fi,
            )

        zero = jnp.zeros(shape, f32)
        last = lax.fori_loop(0, length, one, (zero + 1.0, zero, zero, zero), unroll=2)
        for i in range(4):
            ends[i, :, cols] = last[i]

    def link(earlier, later):
        return (
            later[0] * earlier[0] - later[1] * earlier[1] + later[2],
            later[0] * earlier[1] + later[1] * earlier[0] + later[3],
        )

    def chain(first, second):
        fr, fi, ur, ui = first
        qr, qi, tr, ti = second
        vr, vi = link((ur, ui), second)
        return qr * fr - qi * fi, qr * fi + qi * fr, vr, vi

    def four(ref, *at):
        return tuple(ref[(*at, slice(i, i + 1), slice(None))] for i in range(4))

    whole_run = tuple(ends[i, 0:1, :] for i in range(4))
    for s in range(1, segments):
        whole_run = chain(whole_run, tuple(ends[i, s : s + 1, :] for i in range(4)))
    for i, v in enumerate(whole_run):
        mate[y, i : i + 1, :] = v

    def mate_copy(sending):
        slot = y if sending else 1 - y
        return pltpu.make_async_remote_copy(
            src_ref=mate.at[slot],
            dst_ref=mate.at[slot],
            send_sem=carry_send.at[0],
            recv_sem=carry_recv.at[0],
            device_id=(2 * z + 1 - y, tp),
            device_id_type=MESH,
        )

    def carry_copy(i, sending):
        slot = z if sending else (z + nz - i) % nz
        return pltpu.make_async_remote_copy(
            src_ref=carries.at[slot],
            dst_ref=carries.at[slot],
            send_sem=carry_send.at[i],
            recv_sem=carry_recv.at[i],
            device_id=(2 * ((z + i) % nz) + y, tp),
            device_id_type=MESH,
        )

    upper = z // (nz // 2)

    def second_sends():
        @pl.when(inner == 1)
        def _():
            z_start(0, beyond, early)

        @pl.when(inner == 0)
        def _():
            z_start(0, beyond, 0, before)

    pl.when(upper == 1)(second_sends)
    mate_copy(True).start()
    for part in range(pieces):
        y_copy(1, 0, z, part, True).start()
    mate_copy(False).wait_recv()
    for i, v in enumerate(chain(four(mate, 0), four(mate, 1))):
        carries[z, i : i + 1, :] = v
    for i in range(1, nz):

        @pl.when(z + i < nz)
        def _():
            carry_copy(i, True).start()

    prefix[...] = jnp.zeros_like(prefix)

    def extend(run):
        for i, v in enumerate(link((prefix[0:1, :], prefix[1:2, :]), run)):
            prefix[i : i + 1, :] = v

    for i in range(1, nz):

        @pl.when(z >= i)
        def _():
            carry_copy(i, False).wait_recv()

    for i in range(1, nz):

        @pl.when(z + i < nz)
        def _():
            carry_copy(i, True).wait_send()

    pl.when(upper == 0)(second_sends)

    for d in range(nz - 1):

        @pl.when(d < z)
        def _():
            extend(four(carries, d))

    @pl.when(y == 1)
    def _():
        extend(four(mate, 0))

    cr, ci = prefix[0:1, :], prefix[1:2, :]
    for s in range(segments):
        entry[0, s : s + 1, :] = cr
        entry[1, s : s + 1, :] = ci
        cr, ci = link((cr, ci), tuple(ends[i, s : s + 1, :] for i in range(4)))
    forward(0, 1, pair_z)
    half_way = pieces // 2
    for k, zk in near:
        forward(0, k, zk, 0, half_way)

    for c in range(chunks):
        cols = pl.ds(c * lanes, lanes)

        def again(j, state):
            rows = pl.ds(pl.multiple_of(j * segments, segments), segments)
            dr, di = dre[rows, cols], dim[rows, cols]
            xr, xi = link(state, (dr, di, fre[rows, cols], fim[rows, cols]))
            proj[rows, 0:lanes] = xr
            proj[rows, lanes : 2 * lanes] = xi
            return xr, xi

        lax.fori_loop(0, length, again, (entry[0, :, cols], entry[1, :, cols]), unroll=4)
        ins = slice(c * kin, (c + 1) * kin)
        mech = jnp.zeros((tokens, kin), f32)
        for i in range(2):
            matrix = jnp.dot(
                w_out_ref[i, c * kin : (c + 1) * kin, :].astype(bf16),
                over_states.astype(bf16),
                preferred_element_type=f32,
            )
            mech += (1 - 2 * i) * lax.dot_general(
                proj[:, i * lanes : (i + 1) * lanes].astype(bf16),
                (matrix * agree).astype(bf16),
                (((1,), (1,)), ((), ())),
                preferred_element_type=f32,
            )
        mech = mech + skip_ref[0:1, ins] * mixer_perm[:, ins].astype(f32)
        mixed = jax.nn.gelu(mech).astype(bf16)
        chan[tp, :, ins] = jnp.dot(
            unperm_ref[...], mixed, preferred_element_type=f32
        ).astype(bf16)
        chan_core(0, c, True).start()
        for i in range(1, nx):
            chan_x(i, c, True).start()
        if c >= 2:
            chan_forward(c - 2)

    for c in range(max(chunks - 2, 0), chunks):
        chan_forward(c)
    for c in gates:
        c.wait()
    for c in range(chunks):
        for i in range(nx):
            chan_core(i, c, False).wait_recv()

    tile = 256

    @pl.loop(0, width // tile)
    def _(t):
        cols = pl.ds(pl.multiple_of(t * tile, tile), tile)
        v = jnp.zeros((tokens, tile), f32)
        g = jnp.zeros((tokens, tile), f32)
        for q in range(ntp):
            rows = slice(q * width, (q + 1) * width)
            v += jnp.dot(chan[q], value_ref[rows, cols], preferred_element_type=f32)
            g += jnp.dot(chan[q], gate_ref[rows, cols], preferred_element_type=f32)
        upd[0, tp, :, cols] = (resid_ref[:, cols].astype(f32) + v * jax.nn.sigmoid(g)).astype(bf16)

    def upd_z():
        return pltpu.make_async_remote_copy(
            src_ref=upd.at[0, tp],
            dst_ref=upd.at[1, tp],
            send_sem=upd_z_send.at[0],
            recv_sem=upd_z_recv.at[0],
            device_id=(pair, tp),
            device_id_type=MESH,
        )

    def upd_x(i, h, sending):
        slot = tp if sending else tp_at((x + nx - i) % nx, core)
        return pltpu.make_async_remote_copy(
            src_ref=upd.at[h, slot],
            dst_ref=upd.at[h, slot],
            send_sem=upd_x_send.at[i - 1, h],
            recv_sem=upd_x_recv.at[i - 1, h],
            device_id=(sp, tp_at((x + i) % nx, core)),
            device_id_type=MESH,
        )

    def upd_core(i, h, sending):
        slot = tp_at((x + nx - i) % nx, core if sending else 1 - core)
        return pltpu.make_async_remote_copy(
            src_ref=upd.at[h, slot],
            dst_ref=upd.at[h, slot],
            send_sem=upd_core_send.at[i, h],
            recv_sem=upd_core_recv.at[i, h],
            device_id=(sp, partner),
            device_id_type=MESH,
        )

    upd_z().start()
    for i in range(1, nx):
        upd_x(i, 0, True).start()
    upd_core(0, 0, True).start()

    @pl.when(inner == 0)
    def _():
        z_start(0, beyond, before)
        for k in beyond:
            z_start(1, (k,))
        z_start(1, (1,), ahead)

    @pl.when(inner == 1)
    def _():
        z_start(1, beyond, 0, quarter)
        z_start(1, (1,), 0)

    most = (3 * pieces) // 4
    for k, zk in distant:
        forward(0, k, zk, 0, most)
    for k, zk in near:
        forward(0, k, zk, half_way)
    for i in range(1, nx):
        upd_x(i, 0, False).wait_recv()
        upd_core(i, 0, True).start()
    upd_z().wait_recv()
    for i in range(1, nx):
        upd_x(i, 1, True).start()
    upd_core(0, 1, True).start()
    for k, zk in distant:
        forward(0, k, zk, most)

    def normalize(h):
        for i in range(nx):
            upd_core(i, h, False).wait_recv()
        total = jnp.zeros((tokens, 1), f32)
        for q in range(ntp):
            u = upd[h, q].astype(f32)
            total += jnp.sum(u * u, axis=1, keepdims=True)
        inv = lax.rsqrt(total * (1.0 / (width * ntp)) + rms_eps)
        for q in range(ntp):
            cols = slice(q * width, (q + 1) * width)
            normed[h * tokens : (h + 1) * tokens, cols] = (upd[h, q].astype(f32) * inv * gain_ref[0:1, cols]).astype(bf16)

    normalize(0)
    for i in range(1, nx):
        upd_x(i, 1, False).wait_recv()
        upd_core(i, 1, True).start()
    normalize(1)

    @pl.when(inner == 1)
    def _():
        forward(1, 1, pair_z, 0, ahead)

    @pl.when(inner == 0)
    def _():
        forward(1, 1, pair_z)

    for c in own:
        c.wait()
    y_arrived(0, 0, z)
    y_arrived(0, 1, pair_z)
    for k, zk in far:
        y_arrived(0, k, zk)

    @pl.loop(0, units // tile)
    def _(t):
        cols = pl.ds(pl.multiple_of(t * tile, tile), tile)
        for h in range(2):
            some = slice(h * tokens, (h + 1) * tokens)
            r = jnp.dot(normed[some, :], up_whole[:, cols], preferred_element_type=f32)
            r = jnp.maximum(r, 0.0)
            hidden[some, cols] = (r * r).astype(bf16)

    cuts = sum1_send.shape[1]
    cut = block // cuts

    def strip(h):
        return slice(h * cut, (h + 1) * cut)

    def sum1(s, h):
        return pltpu.make_async_remote_copy(
            src_ref=out1.at[s, :, pl.ds(h * cut, cut)],
            dst_ref=in1.at[s, :, pl.ds(h * cut, cut)],
            send_sem=sum1_send.at[s, h],
            recv_sem=sum1_recv.at[s, h],
            device_id=(sp, partner),
            device_id_type=MESH,
        )

    def sum2(s, h):
        return pltpu.make_async_remote_copy(
            src_ref=out2.at[s, :, pl.ds(h * cut, cut)],
            dst_ref=in2.at[s, :, pl.ds(h * cut, cut)],
            send_sem=sum2_send.at[s, h],
            recv_sem=sum2_recv.at[s, h],
            device_id=(pair, tp),
            device_id_type=MESH,
        )

    def sum3(s, h, there, to):
        return pltpu.make_async_remote_copy(
            src_ref=out3.at[s, :, pl.ds(h * cut, cut)],
            dst_ref=in3.at[s % per, there, :, pl.ds(h * cut, cut)],
            send_sem=sum3_send.at[s, h],
            recv_sem=sum3_recv.at[s % per, there, h],
            device_id=(sp, to),
            device_id_type=MESH,
        )

    def core_of(s):
        return (s // per) % 2

    def x_of(s):
        return s // per // 2

    def stage1(s, first=0, last=cuts):
        rows = pl.ds(pl.multiple_of(s * block + first * cut, cut), (last - first) * cut)

        @pl.loop(0, 2)
        def _(half):
            some = pl.ds(pl.multiple_of(half * tokens, tokens), tokens)
            keep[s, some, first * cut : last * cut] = lax.dot_general(
                hidden[some, :],
                down_whole[rows, :],
                (((1,), (1,)), ((), ())),
                preferred_element_type=f32,
            )

        @pl.when(core_of(s) != core)
        def _():
            for h in range(first, last):
                out1[s, :, strip(h)] = keep[s, :, strip(h)].astype(bf16)
                sum1(s, h).start()

    def stage2(s, first=0, last=cuts):
        @pl.when(core_of(s) == core)
        def _():
            for h in range(first, last):
                w = strip(h)
                sum1(s, h).wait_recv()
                out2[s, :, w] = (keep[s, tokens:, w] + in1[s, tokens:, w].astype(f32)).astype(bf16)
                sum2(s, h).start()
                keep[s, :tokens, w] = keep[s, :tokens, w] + in1[s, :tokens, w].astype(f32)

    def stage3(s, first=0, last=cuts):
        @pl.when(core_of(s) == core)
        def _():
            for h in range(first, last):
                w = strip(h)
                sum2(s, h).wait_recv()
                total = keep[s, :tokens, w] + in2[s, :, w].astype(f32)

                @pl.when(x_of(s) == x)
                def _():
                    keep[s, :tokens, w] = total

                @pl.when(x_of(s) != x)
                def _():
                    out3[s, :, w] = total.astype(bf16)
                    sum3(s, h, x, s // per).start()

    def step(k, zk, side, eager=False):
        if side == 1:
            y_arrived(1, k, zk)
        s = 2 * zk + (y if side == 0 else 1 - y)
        stage1(s)
        if waiting:
            stage2(waiting.pop())
        if eager:
            stage2(s)
        else:
            waiting.append(s)
        order.append(s)

    order, waiting = [], []

    def weights_sent(which):
        slot = wholes[which].at[rows_of(sp)]
        for k in range(nz):
            for sem in (y_send, z_send)[: 1 + (k > 0)]:
                pltpu.make_async_remote_copy(
                    src_ref=slot,
                    dst_ref=slot,
                    send_sem=sem.at[which, k],
                    recv_sem=z_recv.at[which, k, 0],
                    device_id=(2 * z + 1 - y, tp),
                    device_id_type=MESH,
                ).wait_send()

    def first_sent():
        weights_sent(0)
        mate_copy(True).wait_send()
        for i in range(nx):
            for c in range(chunks):
                chan_core(i, c, True).wait_send()
                if i > 0:
                    chan_x(i, c, True).wait_send()
            for h in range(2):
                upd_core(i, h, True).wait_send()
                if i > 0:
                    upd_x(i, h, True).wait_send()
        upd_z().wait_send()

    for k, zk in distant:
        forward(1, k, zk, 0, half_way)
    for side in range(2):
        step(0, z, side)

    @pl.when(inner == 1)
    def _():
        z_start(1, beyond, quarter)

    for k, zk in distant:
        forward(1, k, zk, half_way)

    for k, zk in near:
        forward(1, k, zk, 0, pieces // 4)
    for k, zk in distant:
        for side in range(2):
            step(k, zk, side)
    stage2(waiting.pop())

    @pl.when(inner == 1)
    def _():
        forward(1, 1, pair_z, ahead)

    for k, zk in near:
        forward(1, k, zk, pieces // 4, half_way)
    step(1, pair_z, 0, True)
    for k, zk in near:
        forward(1, k, zk, half_way, most)
    for s in order[2:-1]:
        stage3(s)
    step(1, pair_z, 1, True)
    first_sent()
    for k, zk in near:
        forward(1, k, zk, most)
    remaining = order[:2] + order[-2:]
    ending = []
    for k, zk in near:
        step(k, zk, 0, True)
        ending.append(2 * zk + y)
    for h in range(cuts):
        for k, zk in near:
            for part in range(h * pieces // cuts, (h + 1) * pieces // cuts):
                y_copy(1, k, zk, part, False).wait_recv()
            s = 2 * zk + 1 - y
            stage1(s, h, h + 1)
            stage2(s, h, h + 1)
        if h == 0:
            for e in remaining + ending:
                stage3(e)
    weights_sent(1)
    for s in range(n):

        @pl.when(core_of(s) != core)
        def _():
            for h in range(cuts):
                sum1(s, h).wait_send()

    for h in range(cuts):
        for _, zk in near:
            stage3(2 * zk + 1 - y, h, h + 1)
    for s in range(n):

        @pl.when(core_of(s) == core)
        def _():
            for h in range(cuts):
                sum2(s, h).wait_send()

    for j in range(per):
        s = tp * per + j
        cols = slice(j * block, (j + 1) * block)
        total = keep[s, :tokens]
        for i in range(1, nx):
            there = (x + i) % nx
            for h in range(cuts):
                sum3(s, h, there, tp_at(there, core)).wait_recv()
            total += in3[j, there].astype(f32)
        out_ref[:, cols] = (upd[0, tp, :, cols].astype(f32) + total).astype(bf16)

    for s in range(n):

        @pl.when((core_of(s) == core) & (x_of(s) != x))
        def _():
            for h in range(cuts):
                sum3(s, h, x, s // per).wait_send()


def per_device(
    n,
    ntp,
    resid,
    mixer_in,
    log_step,
    decay_real,
    frequency,
    input_matrix,
    output_matrix,
    skip_gain,
    value_weight,
    gate_weight,
    norm_gain,
    up_weight,
    down_weight,
):
    tokens, width = mixer_in.shape
    groups, states = decay_real.shape
    each = width // groups
    bunch = min(128 // each, groups)
    chunks = groups // bunch
    lanes = bunch * states
    features, units = value_weight.shape[0], up_weight.shape[1] // 2
    block = up_weight.shape[0]
    length = tokens // segments
    row = np.arange(tokens)
    perm = (row[None, :] == ((row % segments) * length + row // segments)[:, None]).astype(np.float32)
    nz, nx, per, pieces = n // 2, ntp // 2, n // ntp, 4
    total = groups * states
    cuts = 2 if block % 256 == 0 else 1
    dma = pltpu.SemaphoreType.DMA
    vmem = pl.BlockSpec(memory_space=pltpu.VMEM)
    hbm = pl.BlockSpec(memory_space=pl.ANY)
    return pl.pallas_call(
        functools.partial(kernel, n, ntp),
        out_shape=jax.ShapeDtypeStruct((tokens, width), bf16),
        in_specs=[vmem] * 8 + [hbm] * 2 + [vmem] + [hbm] * 2 + [vmem] * 2,
        out_specs=vmem,
        scratch_shapes=[
            pltpu.VMEM((features, units), bf16),
            pltpu.VMEM((features, units), bf16),
            pltpu.VMEM((features, width), bf16),
            pltpu.VMEM((features, width), bf16),
            pltpu.VMEM((tokens, total), f32),
            pltpu.VMEM((tokens, total), f32),
            pltpu.VMEM((tokens, total), f32),
            pltpu.VMEM((tokens, total), f32),
            pltpu.VMEM((tokens, lanes), f32),
            pltpu.VMEM((tokens, 2 * lanes), f32),
            pltpu.VMEM((4, segments, total), f32),
            pltpu.VMEM((nz, 4, total), f32),
            pltpu.VMEM((2, 4, total), f32),
            pltpu.VMEM((2, total), f32),
            pltpu.VMEM((2, segments, total), f32),
            pltpu.VMEM((tokens, width), bf16),
            pltpu.VMEM((ntp, tokens, width), bf16),
            pltpu.VMEM((2, ntp, tokens, width), bf16),
            pltpu.VMEM((2 * tokens, features), bf16),
            pltpu.VMEM((2 * tokens, units), bf16),
            pltpu.VMEM((n, 2 * tokens, block), f32),
            pltpu.VMEM((n, 2 * tokens, block), bf16),
            pltpu.VMEM((n, 2 * tokens, block), bf16),
            pltpu.VMEM((n, tokens, block), bf16),
            pltpu.VMEM((n, tokens, block), bf16),
            pltpu.VMEM((n, tokens, block), bf16),
            pltpu.VMEM((per, nx, tokens, block), bf16),
            dma((4,)),
            dma((2, nz)),
            dma((2, nz, pieces)),
            dma((2, nz)),
            dma((2, nz, pieces)),
            dma((nz,)),
            dma((nz,)),
            dma((nx, chunks)),
            dma((nx, chunks)),
            dma((max(nx - 1, 1), chunks)),
            dma((max(nx - 1, 1), chunks)),
            dma((1,)),
            dma((1,)),
            dma((nx, 2)),
            dma((nx, 2)),
            dma((max(nx - 1, 1), 2)),
            dma((max(nx - 1, 1), 2)),
            dma((n, cuts)),
            dma((n, cuts)),
            dma((n, cuts)),
            dma((n, cuts)),
            dma((n, cuts)),
            dma((per, nx, cuts)),
        ],
        compiler_params=pltpu.CompilerParams(
            collective_id=0, has_side_effects=True, vmem_limit_bytes=64 * 1024 * 1024 - 65536
        ),
    )(
        resid,
        mixer_in,
        log_step.T,
        decay_real,
        frequency,
        jnp.transpose(input_matrix, (0, 1, 3, 2)).reshape(2, width, states),
        output_matrix.reshape(2, width, states),
        skip_gain.reshape(1, width),
        value_weight,
        gate_weight,
        norm_gain.reshape(1, features),
        up_weight,
        down_weight,
        jnp.asarray(perm, bf16),
        jnp.asarray(perm.T, bf16),
    )


def solution(mesh):
    in_specs = (
        P("sp", "tp"),
        P("sp", "tp"),
        P("sp", "tp"),
        P("tp", None),
        P("tp", None),
        P(None, "tp", None, None),
        P(None, "tp", None, None),
        P("tp"),
        P(None, "tp"),
        P(None, "tp"),
        P(),
        P("sp", "tp"),
        P("sp", "tp"),
    )
    body = functools.partial(per_device, mesh.shape["sp"], mesh.shape["tp"])
    return jax.shard_map(
        body, mesh=mesh, in_specs=in_specs, out_specs=P("sp", "tp"), check_vma=False
    )
```
